512 devices in a mesh: sp: 64 (over z, y), tp: 8 (over x, core).
Axes of the slice: x: 4, y: 4, z: 16, core: 2. Of those that a mesh axis runs over, the one named last changes fastest.
Arguments:
- block_source: bfloat16 [8192, 2048], P('sp'), may hold values from -28 to 28
- address_weights: bfloat16 [1024, 2048], P('tp'), may hold values from -0.125 to 0.125
- causal_filter_taps: float32 [4, 1024], P(None, 'tp'), may hold values from -3 to 3
- payload_vectors: bfloat16 [8192, 2048], P('sp', 'tp'), may hold values from -0.125 to 0.125
- probe_vectors: bfloat16 [8192, 1024], P('sp', 'tp'), may hold values from -0.5 to 0.5
- interval_preimage: float32 [8192, 32], P('sp', 'tp'), may hold values from -3.5 to 4
- channel_damping_exponent: float32 [32], P('tp'), may hold values from -14 to -3
- added_damping_jumps: float32 [8192, 32], P('sp', 'tp'), may hold values from -1 to 0
- sigmoid_argument: bfloat16 [8192, 2048], P('sp', 'tp'), may hold values from -6 to 6
- adjoint_of_result: bfloat16 [8192, 2048], P('sp', 'tp'), may hold values from -6 to 6
Outputs:
- key_weight_grad: float32 [1024, 2048], P('tp', 'sp')
- row_squares: float32 [1024], P('tp')
- input_grad: bfloat16 [2048, 8192], P('tp', 'sp')
- value_grad: bfloat16 [8192, 2048], P('sp', 'tp')
- query_grad: bfloat16 [8192, 1024], P('sp', 'tp')
- decay_grad: float32 [8192, 32], P('sp', 'tp')
- gate_grad: bfloat16 [8192, 2048], P('sp', 'tp')
The draws below stay inside these ranges and needn't reach their ends.
All inputs are finite; a program needn't handle non-finite values.
Results may differ from the reference program's by a relative error of at most 0.015.
Values may be sent and summed in bfloat16 or wider, within the bound.
No kernel may reach another device: no remote copies, remote signals or barrier semaphores. Data moves between devices by JAX's collectives and lax.ppermute only.
A program may use at most 64 MiB of HBM per device.

```python
import math
import jax
import jax.numpy as jnp
from jax import lax

D = 2048
HEADS = 32
HEAD_DIM = 64
GROUPS = 8
STATE = 128
KCONV = 4
BLOCK = 128
TOK_DEV = 128
TOKENS = 8192
INNER = 2048
KEY_WIDTH = 1024
N_TP = 8


def draw_block_source(key, part):
    base_key, scale_key = jax.random.split(jax.random.fold_in(key, 101), 2)
    column = 3.0 ** (jnp.arange(D, dtype=jnp.float32) / D)
    column = column * jnp.exp(jax.random.uniform(scale_key, (D,), jnp.float32, -0.6, 0.6))
    noise = jnp.clip(jax.random.normal(base_key, (TOKENS, D), jnp.float32), -4.0, 4.0)
    return (noise * column[None]).astype(jnp.bfloat16)


def draw_interval_preimage(key, part):
    level_key, noise_key = jax.random.split(jax.random.fold_in(key, 202), 2)
    block_total = TOKENS // TOK_DEV
    levels = jax.random.uniform(level_key, (block_total, 1), jnp.float32, -1.0, 1.5)
    levels = jnp.repeat(levels, TOK_DEV, axis=0)
    noise = 0.7 * jnp.clip(jax.random.normal(noise_key, (TOKENS, HEADS), jnp.float32), -3.5, 3.5)
    return levels + noise


def draw_channel_damping_exponent(key, part):
    pick_key, slow_key, fast_key = jax.random.split(jax.random.fold_in(key, 303), 3)
    fast_share = 0.5
    slow_low = math.log(0.3 / TOKENS)
    slow_high = math.log(1.0 / 64.0)
    is_fast = jax.random.uniform(pick_key, (HEADS,), jnp.float32) < fast_share
    slow_rate = jnp.exp(jax.random.uniform(slow_key, (HEADS,), jnp.float32, slow_low, slow_high))
    fast_rate = jnp.exp(jax.random.uniform(fast_key, (HEADS,), jnp.float32, math.log(0.01), math.log(0.04)))
    return jnp.log(jnp.where(is_fast, fast_rate, slow_rate))


def draw_added_damping_jumps(key, part):
    spot_key, size_key = jax.random.split(jax.random.fold_in(key, 404), 2)
    spots = jax.random.randint(spot_key, (2, HEADS), 0, TOKENS)
    amounts = jax.random.uniform(size_key, (2, HEADS), jnp.float32, -0.5, -0.22)
    positions = jnp.arange(TOKENS, dtype=jnp.int32)[:, None]
    first = jnp.where(positions == spots[0][None], amounts[0][None], 0.0)
    second = jnp.where(positions == spots[1][None], amounts[1][None], 0.0)
    return (first + second).astype(jnp.float32)


def level_of(rng, dims, pieces, least, top_value):
    level, own = 1.0, jax.random.fold_in(rng, 6)
    for dim, shards_of in pieces:
        heights = jnp.exp(jax.random.uniform(jax.random.fold_in(own, dim), (shards_of,), jnp.float32, least / len(pieces), top_value / len(pieces)))
        level = level * jnp.repeat(heights, dims[dim] // shards_of).reshape([-1 if axis == dim else 1 for axis in range(len(dims))])
    return level


def scatter_about(own_key, extent, spread, reach, cuts=(), held_as=jnp.bfloat16):
    drawn = jax.random.normal(own_key, extent, jnp.float32) * spread
    if len(cuts) > 0:
        drawn = level_of(own_key, extent, cuts, -0.22, 0.18) * drawn
    return jnp.clip(drawn, min=-reach, max=reach).astype(held_as)


def setup_inputs(seed: int = 0) -> dict:
    arg_keys = jax.random.split(jax.random.key(seed), 11)
    return {
        "block_source": draw_block_source(jax.random.fold_in(arg_keys[10], 71), 0),
        "address_weights": scatter_about(arg_keys[1], (KEY_WIDTH, D), D ** -0.5, 0.125, ((0, 8),)),
        "causal_filter_taps": scatter_about(arg_keys[2], (KCONV, KEY_WIDTH), 0.5, 3.0, ((1, 8),), jnp.float32),
        "payload_vectors": scatter_about(arg_keys[3], (TOKENS, INNER), (TOKENS // 4) ** -0.5, 0.125, ((0, 64), (1, 8))),
        "probe_vectors": scatter_about(arg_keys[4], (TOKENS, KEY_WIDTH), STATE ** -0.5, 0.5, ((0, 64), (1, 8))),
        "interval_preimage": draw_interval_preimage(jax.random.fold_in(arg_keys[10], 71), 0),
        "channel_damping_exponent": draw_channel_damping_exponent(jax.random.fold_in(arg_keys[10], 71), 0),
        "added_damping_jumps": draw_added_damping_jumps(jax.random.fold_in(arg_keys[10], 71), 0),
        "sigmoid_argument": scatter_about(arg_keys[8], (TOKENS, INNER), 1.0, 6.0, ((0, 64), (1, 8))),
        "adjoint_of_result": scatter_about(arg_keys[9], (TOKENS, INNER), 1.0, 6.0, ((0, 64), (1, 8))),
    }


HIGHEST = lax.Precision.HIGHEST

def silu_slope(pre_act):
    sigma = jax.nn.sigmoid(pre_act)
    return sigma * (1.0 + pre_act * (1.0 - sigma))

def causal_conv(padded, causal_filter_taps, tokens):
    result = causal_filter_taps[0][None] * padded[0:tokens]
    for offset in range(1, causal_filter_taps.shape[0]):
        result = result + causal_filter_taps[offset][None] * padded[offset:offset + tokens]
    return result

def conv_transpose(extended, causal_filter_taps, tokens):
    tap_count = causal_filter_taps.shape[0]
    result = causal_filter_taps[0][None] * extended[tap_count - 1:tap_count - 1 + tokens]
    for offset in range(1, tap_count):
        first_row = tap_count - 1 - offset
        result = result + causal_filter_taps[offset][None] * extended[first_row:first_row + tokens]
    return result

def block_step(carry_state, inputs):
    payload_vectors, damping_exponent, key_block, probe_vectors, step_block = inputs
    block_len = payload_vectors.shape[0]
    scaled = payload_vectors * step_block[..., None]
    cumulative = jnp.cumsum(damping_exponent, axis=0)
    causal = jnp.tril(jnp.ones((block_len, block_len), dtype=bool))
    gaps = cumulative[:, None] - cumulative[None, :]
    decay_mat = jnp.exp(jnp.where(causal[:, :, None, None], gaps, -jnp.inf))
    scores = jnp.einsum('ign,jgn->gij', probe_vectors, key_block, precision=HIGHEST)
    within = jnp.einsum('gij,ijgr,jgrp->igrp', scores, decay_mat, scaled, precision=HIGHEST)
    carried = jnp.einsum('ign,grpn->igrp', probe_vectors, carry_state, precision=HIGHEST) * jnp.exp(cumulative)[..., None]
    end_decay = cumulative[-1]
    weights = jnp.exp(end_decay[None] - cumulative)
    new_state = carry_state * jnp.exp(end_decay)[..., None, None] + jnp.einsum('jgn,jgr,jgrp->grpn', key_block, weights, scaled, precision=HIGHEST)
    return (new_state, within + carried)

def linear_scan_update(payload_vectors, interval_preimage, pooled_addresses, pooled_probes, starting_memory, channel_damping_exponent, added_damping_jumps):
    tokens = pooled_addresses.shape[0]
    groups = pooled_addresses.shape[1]
    head_count = interval_preimage.shape[1]
    group_heads = head_count // groups
    block_count = tokens // BLOCK
    interval_widths = jax.nn.softplus(interval_preimage)
    damping_exponent = added_damping_jumps - jnp.exp(channel_damping_exponent)[None] * interval_widths

    def to_blocks(array):
        return array.reshape((block_count, BLOCK) + array.shape[1:])
    final_state, outputs = lax.scan(block_step, starting_memory, (to_blocks(payload_vectors.reshape(tokens, groups, group_heads, -1)), to_blocks(damping_exponent.reshape(tokens, groups, group_heads)), to_blocks(pooled_addresses), to_blocks(pooled_probes), to_blocks(interval_widths.reshape(tokens, groups, group_heads))))
    return (outputs.reshape(tokens, -1), final_state)

def reference(block_source, address_weights, causal_filter_taps, payload_vectors, probe_vectors, interval_preimage, channel_damping_exponent, added_damping_jumps, sigmoid_argument, adjoint_of_result):
    tokens = block_source.shape[0]
    channels = address_weights.shape[0]
    projected = jnp.dot(block_source, address_weights.T, preferred_element_type=jnp.float32).astype(jnp.bfloat16)
    padded = jnp.concatenate([jnp.zeros((KCONV - 1, channels), jnp.bfloat16), projected], axis=0).astype(jnp.float32)
    convolved = causal_conv(padded, causal_filter_taps, tokens)
    pooled_addresses = lax.optimization_barrier(jax.nn.silu(convolved).astype(jnp.bfloat16)).astype(jnp.float32)
    pooled_addresses = pooled_addresses.reshape(tokens, GROUPS, STATE)
    pooled_probes = probe_vectors.astype(jnp.float32).reshape(tokens, GROUPS, STATE)
    vanishing_start_memory = jnp.zeros((GROUPS, HEADS // GROUPS, HEAD_DIM, STATE), jnp.float32)

    def mixer(payload_factor, interval_argument_factor, address_factor, probe_factor):
        return linear_scan_update(payload_factor, interval_argument_factor, address_factor, probe_factor, vanishing_start_memory, channel_damping_exponent, added_damping_jumps)[0]
    mixer_out, pullback = jax.vjp(mixer, payload_vectors.astype(jnp.float32), interval_preimage, pooled_addresses, pooled_probes)
    gate_wide = sigmoid_argument.astype(jnp.float32)
    grad_wide = adjoint_of_result.astype(jnp.float32)
    mixed_grad = grad_wide * jax.nn.silu(gate_wide)
    gate_grad = (grad_wide * mixer_out * silu_slope(gate_wide)).astype(jnp.bfloat16)
    value_grad, decay_grad, key_grad, query_grad = pullback(mixed_grad)
    conv_grad = key_grad.reshape(tokens, channels) * silu_slope(convolved)
    extended = jnp.concatenate([conv_grad, jnp.zeros((KCONV - 1, channels), jnp.float32)], axis=0)
    projected_grad = conv_transpose(extended, causal_filter_taps, tokens).astype(jnp.bfloat16)
    key_weight_grad = lax.dot_general(projected_grad, block_source, (((0,), (0,)), ((), ())), preferred_element_type=jnp.float32)
    row_squares = lax.optimization_barrier(jnp.sum(key_weight_grad * key_weight_grad, axis=1))
    range_width = channels // N_TP
    input_total = jnp.zeros((block_source.shape[1], tokens), jnp.float32)
    for tp_rank in range(N_TP):
        low_edge = tp_rank * range_width
        partial_term = lax.dot_general(address_weights[low_edge:low_edge + range_width], projected_grad[:, low_edge:low_edge + range_width], (((0,), (1,)), ((), ())), preferred_element_type=jnp.float32)
        input_total = input_total + lax.optimization_barrier(partial_term.astype(jnp.bfloat16)).astype(jnp.float32)
    input_grad = input_total.astype(jnp.bfloat16)
    return (key_weight_grad, row_squares, input_grad, value_grad.astype(jnp.bfloat16), query_grad.reshape(tokens, channels).astype(jnp.bfloat16), decay_grad, gate_grad)
```

```python
import functools

import jax
import jax.numpy as jnp
from jax import lax
from jax.experimental import pallas as pl
from jax.experimental.pallas import tpu as pltpu
from jax.sharding import Mesh
from jax.sharding import PartitionSpec as P

TOK = 128
STATE = 128
HEAD = 64
R = 4
HP = R * HEAD
Y = 4
NS = STATE // Y
PAD = 8
HIGH = lax.Precision.HIGHEST
F32 = jnp.float32
BF16 = jnp.bfloat16
PALLAS = True
ZY = ("z", "y")


def dot(a, b, ca=1, cb=0, precision=None):
    return lax.dot_general(
        a, b, (((ca,), (cb,)), ((), ())), preferred_element_type=F32, precision=precision
    )


def roll(a, shift):
    size = a.shape[1]
    if PALLAS:
        return pltpu.roll(a, shift % size, 1)
    return jnp.roll(a, shift, axis=1)


def local(fn, outs, *args, flops=10**7):
    single = not isinstance(outs, (list, tuple))
    shapes = [outs] if single else list(outs)
    if not PALLAS:
        res = fn(*args)
        res = [res] if single else list(res)
        for r, s in zip(res, shapes):
            assert r.shape == s.shape and r.dtype == s.dtype, (fn, r, s)
        return res[0] if single else res

    def kernel(*refs):
        ins, dst = refs[: len(args)], refs[len(args) :]
        res = fn(*[r[...] for r in ins])
        res = [res] if single else res
        for ref, val in zip(dst, res):
            ref[...] = val

    vm = pl.BlockSpec(memory_space=pltpu.VMEM)
    res = pl.pallas_call(
        kernel,
        out_shape=shapes,
        in_specs=[vm] * len(args),
        out_specs=[vm] * len(shapes),
        name=fn.__name__,
        cost_estimate=pl.CostEstimate(flops=flops, bytes_accessed=10**6, transcendentals=0),
    )(*args)
    return res[0] if single else res


def sds(shape, dtype):
    return jax.ShapeDtypeStruct(shape, dtype)


def iota2(shape, dim):
    return lax.broadcasted_iota(jnp.int32, shape, dim)


def expand(a):
    return jnp.concatenate(
        [jnp.broadcast_to(a[:, h : h + 1], (a.shape[0], HEAD)) for h in range(R)], axis=1
    )


def split3(a):
    hi = a.astype(BF16)
    rest = a - hi.astype(F32)
    mid = rest.astype(BF16)
    low = (rest - mid.astype(F32)).astype(BF16)
    return hi, mid, low


def joined(parts, first):
    return (
        parts[:, first].astype(F32)
        + parts[:, first + 1].astype(F32)
        + parts[:, first + 2].astype(F32)
    )


def decays(tpre, aexp, jump):
    step = jnp.log(1.0 + jnp.exp(tpre))
    rate = jnp.exp(aexp)
    la = jump - rate * step
    tri = (iota2((TOK, TOK), 0) >= iota2((TOK, TOK), 1)).astype(F32)
    cum = dot(tri, la, precision=HIGH)
    return step, rate, la, cum


def sigmoid(v):
    return 1.0 / (1.0 + jnp.exp(-v))


def bwd_local(tpre, aexp, jump, gate, adj, q):
    step, rate, la, cum = decays(tpre, aexp, jump)
    g = gate.astype(F32)
    dy = adj.astype(F32) * g * sigmoid(g)
    dye = (dy * expand(jnp.exp(cum))).astype(BF16)
    lg = dot(q, dye, 0, 0).astype(BF16)
    hi, mid, low = split3(expand(cum[TOK - 1 :]))
    tail = jnp.concatenate([hi, mid, low, jnp.zeros((PAD - 3, HP), BF16)], axis=0)
    return jnp.stack([jnp.concatenate([lg[NS * i : NS * (i + 1)], tail], axis=0) for i in range(Y)])


def masks_of(cum, cum_t, h):
    causal = iota2((TOK, TOK), 0) >= iota2((TOK, TOK), 1)
    return jnp.exp(jnp.where(causal, cum[:, h : h + 1] - cum_t[h : h + 1, :], -1e30))


def fwd_local(tpre, aexp, jump, gate, adj, q, v, x, w, rim, taps_t):
    step, rate, la, cum = decays(tpre, aexp, jump)
    upper = (iota2((TOK, TOK), 0) <= iota2((TOK, TOK), 1)).astype(F32)
    cum_t = dot(la, upper, 0, 0, HIGH)
    g = gate.astype(F32)
    dy = (adj.astype(F32) * g * sigmoid(g)).astype(BF16)
    u = v.astype(F32) * expand(step)
    ud = (u * expand(jnp.exp(cum[TOK - 1 :] - cum))).astype(BF16)
    u = u.astype(BF16)
    dc = jnp.zeros((TOK, TOK), F32)
    for h in range(R):
        at = slice(HEAD * h, HEAD * (h + 1))
        dc = dc + masks_of(cum, cum_t, h) * dot(dy[:, at], u[:, at], 1, 1)
    dki = dot(q, dc.astype(BF16), 0, 0)
    proj = dot(w, x, 1, 1).astype(BF16).astype(F32)
    rim_proj = dot(w, rim, 1, 1).astype(BF16)
    place = (iota2((PAD, TOK), 1) == iota2((PAD, TOK), 0) + (TOK - PAD)).astype(BF16)
    rim_full = dot(rim_proj, place)
    lane = iota2((STATE, TOK), 1)
    conv = taps_t[:, 3:4] * proj
    for d in range(1, 4):
        conv = conv + taps_t[:, 3 - d : 4 - d] * roll(
            jnp.where(lane >= TOK - d, rim_full, proj), d
        )
    sig = sigmoid(conv)
    keys = (conv * sig).astype(BF16)
    slope = sig * (1.0 + conv * (1.0 - sig))
    ls = dot(keys, ud).astype(BF16)
    pair = jnp.concatenate([dki.astype(BF16), slope.astype(BF16)], axis=1)
    chunks = [rim[:, HP * i : HP * (i + 1)] for i in range(rim.shape[1] // HP)]
    shared = jnp.concatenate([ud] + chunks, axis=0)
    mid = jnp.stack(
        [
            jnp.concatenate(
                [shared, ls[NS * i : NS * (i + 1)], pair[NS * i : NS * (i + 1)]], axis=0
            )
            for i in range(Y)
        ]
    )
    return mid, keys


def bwd_group(got):
    tau = joined(got, NS)
    acc = got[Y - 1, :NS].astype(F32)
    for j in range(Y - 2, -1, -1):
        acc = got[j, :NS].astype(F32) + jnp.exp(tau[j : j + 1]) * acc
    hi, mid, low = split3(jnp.sum(tau, axis=0, keepdims=True))
    return jnp.concatenate(
        [acc.astype(BF16), hi, mid, low, jnp.zeros((PAD - 3, HP), BF16)], axis=0
    )


def fwd_group(got, mid):
    tau = joined(got, NS)
    at = slice(TOK + 8 * PAD, TOK + 8 * PAD + NS)
    acc = mid[0, at].astype(F32)
    for j in range(1, Y):
        acc = mid[j, at].astype(F32) + jnp.exp(tau[j : j + 1]) * acc
    return acc.astype(BF16)


def chain_sums(far):
    count = far.shape[0]
    tau = joined(far, NS)
    tri = (iota2((count, count), 0) >= iota2((count, count), 1)).astype(F32)
    upto = dot(tri, tau, precision=HIGH)
    return tau, upto


def weighted(weights, far):
    acc = weights[0:1] * far[0, :NS].astype(F32)
    for i in range(1, far.shape[0]):
        acc = acc + weights[i : i + 1] * far[i, :NS].astype(F32)
    return acc


def bwd_apply(far, got, mid, xg, taps_own, zrow):
    count = far.shape[0]
    tau, upto = chain_sums(far)
    row = iota2((count, HP), 0)
    mine = jnp.sum(jnp.where(row == zrow, upto, 0.0), axis=0, keepdims=True)
    weights = jnp.exp(jnp.where(row > zrow, upto - tau - mine, -1e30))
    state = weighted(weights, far)
    tau_j = joined(got, NS)
    ends = [None] * Y
    for j in range(Y - 1, -1, -1):
        ends[j] = state.astype(BF16)
        if j:
            state = got[j, :NS].astype(F32) + jnp.exp(tau_j[j : j + 1]) * state
    own = TOK + 8 * PAD + NS
    cg = []
    for j in range(Y):
        dk = dot(ends[j], mid[j, :TOK], 1, 1) + mid[j, own : own + NS, :TOK].astype(F32)
        cg.append(dk * mid[j, own : own + NS, TOK:].astype(F32))
    cg = jnp.concatenate(cg, axis=1)
    size = Y * TOK
    lane = iota2((NS, size), 1)
    main = taps_own[:, 3:4] * cg
    over = jnp.zeros_like(main)
    for d in range(1, 4):
        moved = taps_own[:, 3 - d : 4 - d] * roll(cg, -d)
        main = main + jnp.where(lane < size - d, moved, 0.0)
        over = over + jnp.where(lane >= size - d, moved, 0.0)
    rims = jnp.concatenate(
        [mid[0, TOK + PAD * i : TOK + PAD * (i + 1)] for i in range(8)], axis=1
    )
    over = over[:, size - TOK :]
    zero = jnp.zeros((TOK - PAD, rims.shape[1]), BF16)
    dw = dot(main.astype(BF16), xg) + dot(over.astype(BF16), jnp.concatenate([zero, rims], axis=0))
    width = dw.shape[1] // count
    dw = jnp.stack([dw[:, width * i : width * (i + 1)] for i in range(count)]).astype(BF16)
    return dw, jnp.stack(ends), main, over


def fwd_apply(far, bfar, got, mid, ends, zrow):
    count = far.shape[0]
    tau, upto = chain_sums(bfar)
    row = iota2((count, HP), 0)
    before = jnp.sum(jnp.where(row == zrow, upto - tau, 0.0), axis=0, keepdims=True)
    weights = jnp.exp(jnp.where(row < zrow, before - upto, -1e30))
    state = weighted(weights, far)
    tau_j = joined(got, NS)
    at = slice(TOK + 8 * PAD, TOK + 8 * PAD + NS)
    res = []
    for j in range(Y):
        res.append(jnp.concatenate([state.astype(BF16), ends[j]], axis=0))
        if j < Y - 1:
            state = mid[j, at].astype(F32) + jnp.exp(tau_j[j : j + 1]) * state
    return jnp.stack(res)


def head_sums(a):
    return jnp.concatenate(
        [jnp.sum(a[:, HEAD * h : HEAD * (h + 1)], axis=1, keepdims=True) for h in range(R)], axis=1
    )


def finish(states, tpre, aexp, jump, gate, adj, q, v, keys):
    step, rate, la, cum = decays(tpre, aexp, jump)
    upper = (iota2((TOK, TOK), 0) <= iota2((TOK, TOK), 1)).astype(F32)
    cum_t = dot(la, upper, 0, 0, HIGH)
    s_in = jnp.concatenate([states[i, :NS] for i in range(Y)], axis=0)
    g_out = jnp.concatenate([states[i, NS:] for i in range(Y)], axis=0)
    g = gate.astype(F32)
    a = adj.astype(F32)
    sig = sigmoid(g)
    dy = a * g * sig
    vw = v.astype(F32)
    stepw = expand(step)
    u = vw * stepw
    e = expand(jnp.exp(cum))
    d = expand(jnp.exp(cum[TOK - 1 :] - cum))
    dyb, ub = dy.astype(BF16), u.astype(BF16)
    scores = dot(q, keys)
    y_far = e * dot(q, s_in)
    du_far = d * dot(keys, g_out, 0, 0)
    dc = jnp.zeros((TOK, TOK), F32)
    ys, dus, diffs = [], [], []
    for h in range(R):
        at = slice(HEAD * h, HEAD * (h + 1))
        mask = masks_of(cum, cum_t, h)
        z = dot(dyb[:, at], ub[:, at], 1, 1)
        lz = mask * z
        dc = dc + lz
        m = lz * scores
        diffs.append(jnp.sum(m - m.T, axis=1, keepdims=True))
        lc = (mask * scores).astype(BF16)
        ys.append(dot(lc, ub[:, at]))
        dus.append(dot(lc, dyb[:, at], 0, 0))
    y = y_far + jnp.concatenate(ys, axis=1)
    du = du_far + jnp.concatenate(dus, axis=1)
    from_d = head_sums(u * du_far)
    dcum = jnp.concatenate(diffs, axis=1) + head_sums(dy * y_far) - from_d
    kept = jnp.sum(s_in.astype(F32) * g_out.astype(F32), axis=0, keepdims=True)
    dtot = jnp.sum(from_d, axis=0, keepdims=True) + jnp.exp(cum[TOK - 1 :]) * head_sums(kept)
    dla = dot(upper, dcum, precision=HIGH) + dtot
    dstep = head_sums(du * vw) - rate * dla
    decay_grad = dstep * sigmoid(tpre)
    value_grad = (du * stepw).astype(BF16)
    query_grad = (
        dot(dc.astype(BF16), keys, 1, 1) + dot((dy * e).astype(BF16), s_in, 1, 1)
    ).astype(BF16)
    gate_grad = (a * y * (sig * (1.0 + g * (1.0 - sig)))).astype(BF16)
    return value_grad, query_grad, decay_grad, gate_grad


def summed(parts):
    acc = parts[0].astype(F32)
    for i in range(1, parts.shape[0]):
        acc = acc + parts[i].astype(F32)
    return acc


def weight_sum(parts):
    acc = summed(parts)
    squares = jnp.sum(acc * acc, axis=1, keepdims=True)
    return acc, squares


def exchange(parts, axis):
    return lax.all_to_all(parts, axis, split_axis=0, concat_axis=0, tiled=True)


def copies(part, count):
    return jnp.broadcast_to(part[None], (count, *part.shape))


def per_device(
    block_source,
    address_weights,
    causal_filter_taps,
    payload_vectors,
    probe_vectors,
    interval_preimage,
    channel_damping_exponent,
    added_damping_jumps,
    sigmoid_argument,
    adjoint_of_result,
):
    zs = lax.axis_size("z")
    sp = zs * Y
    tp = lax.axis_size("tp")
    features = block_source.shape[1]
    zi = lax.axis_index("z")
    yi = lax.axis_index("y")
    zrow = jnp.full((1, HP), zi, jnp.int32)
    aexp = channel_damping_exponent.reshape(1, R)
    taps_t = causal_filter_taps.T
    taps_own = lax.dynamic_slice(taps_t, (yi * NS, 0), (NS, taps_t.shape[1]))
    small = (interval_preimage, aexp, added_damping_jumps, sigmoid_argument, adjoint_of_result)
    rim = lax.ppermute(block_source[TOK - PAD :], ZY, [(i, i + 1) for i in range(sp - 1)])
    rim = jnp.where(iota2((PAD, 1), 0) >= PAD - 3, rim, jnp.zeros_like(rim))
    bwd_send = local(bwd_local, sds((Y, NS + PAD, HP), BF16), *small, probe_vectors)
    got = exchange(bwd_send, "y")
    xg = exchange(copies(block_source, Y), "y").reshape(Y * TOK, features)
    rows = TOK + 8 * PAD + 2 * NS
    mid_send, keys = local(
        fwd_local,
        [sds((Y, rows, HP), BF16), sds((STATE, TOK), BF16)],
        *small,
        probe_vectors,
        payload_vectors,
        block_source,
        address_weights,
        rim,
        taps_t,
    )
    mid = exchange(mid_send, "y")
    far = exchange(copies(local(bwd_group, sds((NS + PAD, HP), BF16), got), zs), "z")
    width = features // zs
    dw_send, ends, main, over = local(
        bwd_apply,
        [
            sds((zs, NS, width), BF16),
            sds((Y, NS, HP), BF16),
            sds((NS, Y * TOK), F32),
            sds((NS, TOK), F32),
        ],
        far,
        got,
        mid,
        xg,
        taps_own,
        zrow,
    )
    dw_parts = exchange(dw_send, "z")
    fwd_far = exchange(copies(local(fwd_group, sds((NS, HP), BF16), got, mid), zs), "z")
    state_send = local(
        fwd_apply, sds((Y, 2 * NS, HP), BF16), fwd_far, far, got, mid, ends, zrow
    )
    states = exchange(state_send, "y")
    value_grad, query_grad, decay_grad, gate_grad = local(
        finish,
        [sds((TOK, HP), BF16), sds((TOK, STATE), BF16), sds((TOK, R), F32), sds((TOK, HP), BF16)],
        states,
        *small,
        probe_vectors,
        payload_vectors,
        keys,
    )
    dw, squares = local(weight_sum, [sds((NS, width), F32), sds((NS, 1), F32)], dw_parts)
    squares = jnp.broadcast_to(squares.reshape(1, NS), (sp, NS))
    row_squares = jnp.sum(exchange(squares, ZY).reshape(zs, Y * NS), axis=0)
    pieces = jnp.moveaxis(dw.reshape(NS, Y, width // Y), 1, 0)
    key_weight_grad = exchange(pieces, "y").reshape(Y * NS, width // Y)
    after = lax.ppermute(over, "z", [(i, i - 1) for i in range(1, zs)])
    tokens = jnp.moveaxis(main.reshape(NS, Y, TOK), 1, 0)
    tokens = jnp.concatenate([tokens[: Y - 1], tokens[Y - 1 :] + after[None]], axis=0)
    projected_grad = exchange(tokens.astype(BF16), "y").reshape(STATE, TOK)
    partial = dot(address_weights, projected_grad, 0, 0).astype(BF16)
    input_grad = jnp.sum(
        exchange(partial.reshape(tp, features // tp, TOK), "tp").astype(F32), axis=0
    ).astype(BF16)
    return (
        key_weight_grad,
        row_squares,
        input_grad,
        value_grad,
        query_grad,
        decay_grad,
        gate_grad,
    )


def solution(mesh):
    sp, tp = mesh.shape["sp"], mesh.shape["tp"]
    fine = Mesh(mesh.devices.reshape(sp // Y, Y, tp), ("z", "y", "tp"))
    sh = P(ZY, "tp")
    in_specs = (
        P(ZY, None),
        P("tp", None),
        P(None, "tp"),
        sh,
        sh,
        sh,
        P("tp"),
        sh,
        sh,
        sh,
    )
    out_specs = (P("tp", ZY), P("tp"), P("tp", ZY), sh, sh, sh, sh)
    return jax.shard_map(
        per_device, mesh=fine, in_specs=in_specs, out_specs=out_specs, check_vma=False
    )
```

```python
import jax
import jax.numpy as jnp
from jax import lax
from jax.experimental import pallas as pl
from jax.experimental.pallas import tpu as pltpu
from jax.sharding import Mesh
from jax.sharding import PartitionSpec as P


TOK = 128
STATE = 128
HEAD = 64
R = 4
HP = R * HEAD
Y = 4
NS = STATE // Y
PAD = 8
HIGH = lax.Precision.HIGHEST
F32 = jnp.float32
BF16 = jnp.bfloat16
PALLAS = True
CORES = 2
ZY = ("z", "y")
VMEM_LIMIT = 16 * 2**20


def dot(a, b, ca=1, cb=0, precision=None):
    return lax.dot_general(
        a, b, (((ca,), (cb,)), ((), ())), preferred_element_type=F32, precision=precision
    )


def roll(a, shift):
    size = a.shape[1]
    if PALLAS:
        return pltpu.roll(a, shift % size, 1)
    return jnp.roll(a, shift, axis=1)


def local(fn, outs, *args, flops=10**7, raw=()):
    single = not isinstance(outs, (list, tuple))
    shapes = [outs] if single else list(outs)
    if not PALLAS:
        res = fn(*args)
        res = [res] if single else list(res)
        for r, s in zip(res, shapes):
            assert r.shape == s.shape and r.dtype == s.dtype, (fn, r, s)
        return res[0] if single else res

    def kernel(*refs):
        ins, dst = refs[: len(args)], refs[len(args) :]
        res = fn(*[r if i in raw else r[...] for i, r in enumerate(ins)])
        res = [res] if single else res
        for ref, val in zip(dst, res):
            ref[...] = val

    vm = pl.BlockSpec(memory_space=pltpu.VMEM)
    res = pl.pallas_call(
        kernel,
        out_shape=shapes,
        in_specs=[vm] * len(args),
        out_specs=[vm] * len(shapes),
        cost_estimate=pl.CostEstimate(flops=flops, bytes_accessed=10**6, transcendentals=0),
        compiler_params=pltpu.CompilerParams(vmem_limit_bytes=VMEM_LIMIT),
    )(*args)
    return res[0] if single else res


def sds(shape, dtype):
    return jax.ShapeDtypeStruct(shape, dtype)


def choose(parts, index):
    res = parts[0]
    for i in range(1, len(parts)):
        res = jnp.where(index == i, parts[i], res)
    return res


def to_peers(parts):
    yi = lax.axis_index("y")
    return [choose(parts, lax.rem(yi + d, Y)) for d in range(Y)]


def from_peers(parts):
    yi = lax.axis_index("y")
    return [choose(parts, lax.rem(yi + Y - j, Y)) for j in range(Y)]


def columns_at(ref, start, size):
    if PALLAS:
        return ref[:, pl.ds(pl.multiple_of(start, size), size)]
    return lax.dynamic_slice_in_dim(ref, start, size, axis=1)


def iota2(shape, dim):
    return lax.broadcasted_iota(jnp.int32, shape, dim)


def expand(a):
    return jnp.concatenate(
        [jnp.broadcast_to(a[:, h : h + 1], (a.shape[0], HEAD)) for h in range(R)], axis=1
    )


def split3(a):
    hi = a.astype(BF16)
    rest = a - hi.astype(F32)
    mid = rest.astype(BF16)
    low = (rest - mid.astype(F32)).astype(BF16)
    return hi, mid, low


def joined(parts, first):
    return (
        parts[:, first].astype(F32)
        + parts[:, first + 1].astype(F32)
        + parts[:, first + 2].astype(F32)
    )


def column(a):
    eye = (iota2((TOK, TOK), 0) == iota2((TOK, TOK), 1)).astype(F32)
    return dot(eye, a, 1, 1, HIGH)


def decays(tpre, aexp, jump):
    step = jnp.log(1.0 + jnp.exp(tpre))
    rate = jnp.exp(aexp)
    la = jump - rate * step
    tri = (iota2((TOK, TOK), 0) >= iota2((TOK, TOK), 1)).astype(F32)
    cum = dot(tri, la, 1, 1, HIGH)
    return step, rate, la, cum


def row_form(la):
    upper = (iota2((TOK, TOK), 0) <= iota2((TOK, TOK), 1)).astype(F32)
    return dot(la, upper, precision=HIGH)


def sigmoid(v):
    return 1.0 / (1.0 + jnp.exp(-v))


def bwd_local(tpre, aexp, jump, gate, adj, q):
    cum = decays(tpre, aexp, jump)[3]
    g = gate.astype(F32)
    dy = adj.astype(F32) * g * sigmoid(g)
    dye = (dy * expand(jnp.exp(cum))).astype(BF16)
    lg = dot(q, dye, 0, 0).astype(BF16)
    hi, mid, low = split3(expand(cum[TOK - 1 :]))
    tail = jnp.concatenate([hi, mid, low, jnp.zeros((PAD - 3, HP), BF16)], axis=0)
    return jnp.stack([jnp.concatenate([lg[NS * i : NS * (i + 1)], tail], axis=0) for i in range(Y)])


def masks_of(cum, cum_t, h):
    causal = iota2((TOK, TOK), 0) >= iota2((TOK, TOK), 1)
    return jnp.exp(jnp.where(causal, cum[:, h : h + 1] - cum_t[h : h + 1, :], -1e30))


def fwd_local(tpre, aexp, jump, gate, adj, q, v, x, w, rim, taps):
    step, _, la, cum = decays(tpre, aexp, jump)
    cum_t = row_form(la)
    taps_t = column(taps)
    rim = jnp.where(iota2(rim.shape, 0) >= PAD - 3, rim.astype(F32), 0.0).astype(BF16)
    g = gate.astype(F32)
    dy = (adj.astype(F32) * g * sigmoid(g)).astype(BF16)
    u = v.astype(F32) * expand(column(step))
    ud = (u * expand(jnp.exp(cum[TOK - 1 :] - cum))).astype(BF16)
    u = u.astype(BF16)
    dc = jnp.zeros((TOK, TOK), F32)
    for h in range(R):
        at = slice(HEAD * h, HEAD * (h + 1))
        dc = dc + masks_of(cum, cum_t, h) * dot(dy[:, at], u[:, at], 1, 1)
    dki = dot(q, dc.astype(BF16), 0, 0)
    proj = dot(w, x, 1, 1).astype(BF16).astype(F32)
    rim_proj = dot(w, rim, 1, 1).astype(BF16)
    place = (iota2((PAD, TOK), 1) == iota2((PAD, TOK), 0) + (TOK - PAD)).astype(BF16)
    rim_full = dot(rim_proj, place)
    lane = iota2((STATE, TOK), 1)
    conv = taps_t[:, 3:4] * proj
    for d in range(1, 4):
        conv = conv + taps_t[:, 3 - d : 4 - d] * roll(
            jnp.where(lane >= TOK - d, rim_full, proj), d
        )
    sig = sigmoid(conv)
    keys = (conv * sig).astype(BF16)
    slope = sig * (1.0 + conv * (1.0 - sig))
    ls = dot(keys, ud).astype(BF16)
    pair = jnp.concatenate([dki.astype(BF16), slope.astype(BF16)], axis=1)
    chunks = [rim[:, HP * i : HP * (i + 1)] for i in range(rim.shape[1] // HP)]
    shared = jnp.concatenate([ud] + chunks, axis=0)
    mids = [
        jnp.concatenate([shared, ls[NS * i : NS * (i + 1)], pair[NS * i : NS * (i + 1)]], axis=0)
        for i in range(Y)
    ]
    return *to_peers(mids), keys


def bwd_group(got):
    tau = joined(got, NS)
    acc = got[Y - 1, :NS].astype(F32)
    for j in range(Y - 2, -1, -1):
        acc = got[j, :NS].astype(F32) + jnp.exp(tau[j : j + 1]) * acc
    hi, mid, low = split3(jnp.sum(tau, axis=0, keepdims=True))
    part = jnp.concatenate(
        [acc.astype(BF16), hi, mid, low, jnp.zeros((PAD - 3, HP), BF16)], axis=0
    )
    return jnp.stack([part] * lax.axis_size("z"))


def fwd_group(got, mid):
    tau = joined(got, NS)
    at = slice(TOK + 8 * PAD, TOK + 8 * PAD + NS)
    acc = mid[0][at].astype(F32)
    for j in range(1, Y):
        acc = mid[j][at].astype(F32) + jnp.exp(tau[j : j + 1]) * acc
    return acc.astype(BF16)


def chain_sums(far):
    count = far.shape[0]
    tau = joined(far, NS)
    tri = (iota2((count, count), 0) >= iota2((count, count), 1)).astype(F32)
    upto = dot(tri, tau, precision=HIGH)
    return tau, upto


def weighted(weights, far):
    acc = weights[0:1] * far[0, :NS].astype(F32)
    for i in range(1, far.shape[0]):
        acc = acc + weights[i : i + 1] * far[i, :NS].astype(F32)
    return acc


def bwd_apply(far, got, m0, m1, m2, m3, x0, x1, x2, x3, taps):
    mid = from_peers([m0, m1, m2, m3])
    yi = lax.axis_index("y")
    zrow = lax.axis_index("z")
    mine = iota2((NS, STATE), 1) == iota2((NS, STATE), 0) + NS * lax.axis_index("y")
    taps_own = dot(mine.astype(F32), taps, 1, 1, HIGH)
    count = far.shape[0]
    tau, upto = chain_sums(far)
    row = iota2((count, HP), 0)
    mine = jnp.sum(jnp.where(row == zrow, upto, 0.0), axis=0, keepdims=True)
    weights = jnp.exp(jnp.where(row > zrow, upto - tau - mine, -1e30))
    state = weighted(weights, far)
    tau_j = joined(got, NS)
    ends = [None] * Y
    for j in range(Y - 1, -1, -1):
        ends[j] = state.astype(BF16)
        if j:
            state = got[j, :NS].astype(F32) + jnp.exp(tau_j[j : j + 1]) * state
    own = TOK + 8 * PAD + NS
    cg = []
    for j in range(Y):
        dk = dot(ends[j], mid[j][:TOK], 1, 1) + mid[j][own : own + NS, :TOK].astype(F32)
        cg.append(dk * mid[j][own : own + NS, TOK:].astype(F32))
    cg = jnp.concatenate(cg, axis=1)
    size = Y * TOK
    lane = iota2((NS, size), 1)
    main = taps_own[:, 3:4] * cg
    over = jnp.zeros_like(main)
    for d in range(1, 4):
        moved = taps_own[:, 3 - d : 4 - d] * roll(cg, -d)
        main = main + jnp.where(lane < size - d, moved, 0.0)
        over = over + jnp.where(lane >= size - d, moved, 0.0)
    rims = jnp.concatenate(
        [mid[0][TOK + PAD * i : TOK + PAD * (i + 1)] for i in range(8)], axis=1
    )
    over = over[:, size - TOK :]
    zero = jnp.zeros((TOK - PAD, rims.shape[1]), BF16)
    dw = dot(over.astype(BF16), jnp.concatenate([zero, rims], axis=0))
    pg = main.astype(BF16)
    pg = [pg[:, TOK * i : TOK * (i + 1)] for i in range(Y)]
    for d, part in enumerate((x0, x1, x2, x3)):
        dw = dw + dot(choose(pg, lax.rem(yi + Y - d, Y)), part)
    width = dw.shape[1] // count
    dw = dw.astype(BF16)
    fwd = fwd_group(got, mid)
    send = jnp.stack(
        [
            jnp.concatenate([dw[:, width * i : width * (i + 1)], fwd], axis=1)
            for i in range(count)
        ]
    )
    return send, jnp.stack(ends), main, over


def fwd_apply(near, bfar, got, m0, m1, m2, m3, ends):
    mid = from_peers([m0, m1, m2, m3])
    far = near[:, :, near.shape[2] - HP :]
    zrow = lax.axis_index("z")
    count = far.shape[0]
    tau, upto = chain_sums(bfar)
    row = iota2((count, HP), 0)
    before = jnp.sum(jnp.where(row == zrow, upto - tau, 0.0), axis=0, keepdims=True)
    weights = jnp.exp(jnp.where(row < zrow, before - upto, -1e30))
    state = weighted(weights, far)
    tau_j = joined(got, NS)
    at = slice(TOK + 8 * PAD, TOK + 8 * PAD + NS)
    res = []
    for j in range(Y):
        res.append(jnp.concatenate([state.astype(BF16), ends[j]], axis=0))
        if j < Y - 1:
            state = mid[j][at].astype(F32) + jnp.exp(tau_j[j : j + 1]) * state
    return to_peers(res)


def finish(p0, p1, p2, p3, tpre, aexp, jump, gate, adj, q, v, keys):
    step, rate, la, cum = decays(tpre, aexp, jump)
    cum_t = row_form(la)
    states = from_peers([p0, p1, p2, p3])
    s_in = jnp.concatenate([part[:NS] for part in states], axis=0)
    g_out = jnp.concatenate([part[NS:] for part in states], axis=0)
    g = gate.astype(F32)
    a = adj.astype(F32)
    sig = sigmoid(g)
    dy = a * g * sig
    vw = v.astype(F32)
    stepw = expand(column(step))
    u = vw * stepw
    e = expand(jnp.exp(cum))
    d = expand(jnp.exp(cum[TOK - 1 :] - cum))
    dyb, ub = dy.astype(BF16), u.astype(BF16)
    scores = dot(q, keys)
    y_far = e * dot(q, s_in)
    du_far = d * dot(keys, g_out, 0, 0)
    dc = jnp.zeros((TOK, TOK), F32)
    ys, dus, diffs = [], [], []
    for h in range(R):
        at = slice(HEAD * h, HEAD * (h + 1))
        mask = masks_of(cum, cum_t, h)
        z = dot(dyb[:, at], ub[:, at], 1, 1)
        lz = mask * z
        dc = dc + lz
        m = lz * scores
        diffs.append(jnp.sum(m.T - m, axis=0, keepdims=True))
        lc = (mask * scores).astype(BF16)
        ys.append(dot(lc, ub[:, at]))
        dus.append(dot(lc, dyb[:, at], 0, 0))
    y = y_far + jnp.concatenate(ys, axis=1)
    du = du_far + jnp.concatenate(dus, axis=1)
    pick = (iota2((R, HP), 1) // HEAD == iota2((R, HP), 0)).astype(F32)
    from_d = dot(pick, u * du_far, 1, 1, HIGH)
    dcum = jnp.concatenate(diffs, axis=0) + dot(pick, dy * y_far, 1, 1, HIGH) - from_d
    kept = jnp.sum(s_in.astype(F32) * g_out.astype(F32), axis=0, keepdims=True)
    kept = kept * expand(jnp.exp(cum[TOK - 1 :]))
    dtot = jnp.sum(from_d, axis=1, keepdims=True) + jnp.sum(pick * kept, axis=1, keepdims=True)
    later = (iota2((TOK, TOK), 0) >= iota2((TOK, TOK), 1)).astype(F32)
    dla = dot(dcum, later, precision=HIGH) + dtot
    dstep = dot(pick, du * vw, 1, 1, HIGH) - rate * dla
    decay_grad = dstep * sigmoid(tpre)
    value_grad = (du * stepw).astype(BF16)
    query_grad = (
        dot(dc.astype(BF16), keys, 1, 1) + dot((dy * e).astype(BF16), s_in, 1, 1)
    ).astype(BF16)
    gate_grad = (a * y * (sig * (1.0 + g * (1.0 - sig)))).astype(BF16)
    return value_grad, query_grad, decay_grad, gate_grad


def summed(parts):
    acc = parts[0].astype(F32)
    for i in range(1, parts.shape[0]):
        acc = acc + parts[i].astype(F32)
    return acc


def weight_sum(near):
    acc = summed(near[:, :, : near.shape[2] - HP])
    count = lax.axis_size("z") * Y
    place = iota2((NS, STATE), 1) == iota2((NS, STATE), 0) + NS * lax.axis_index("y")
    placed = dot(acc, place.astype(F32), 0, 0, HIGH)
    width = placed.shape[0] // Y
    pieces = to_peers([placed[width * i : width * (i + 1)] for i in range(Y)])
    squares = jnp.sum(placed * placed, axis=0, keepdims=True)
    return *pieces, jnp.broadcast_to(squares[None], (count, 1, STATE))


def own_tokens(main, after):
    last = Y * TOK - TOK
    whole = jnp.concatenate([main[:, :last], main[:, last:] + after], axis=1).astype(BF16)
    return to_peers([whole[:, TOK * i : TOK * (i + 1)] for i in range(Y)])


def partial_input(w, p0, p1, p2, p3):
    grad = jnp.concatenate(from_peers([p0, p1, p2, p3]), axis=0)
    count = lax.axis_size("tp")
    chips = count // CORES
    width = w.shape[1] // count
    place = lax.axis_index("tp")
    core = lax.rem(place, CORES)
    chip = lax.div(place, CORES)
    res = []
    for side in range(CORES):
        owner = lax.rem(core + side, CORES)
        blocks = []
        for d in range(chips):
            rank = lax.rem(chip + d, chips) * CORES + owner
            blocks.append(dot(columns_at(w, rank * width, width), grad, 0, 0).astype(BF16))
        res.append(jnp.stack(blocks))
    return res


def core_sum(mine, other):
    return [
        (mine[i].astype(F32) + other[i].astype(F32)).astype(BF16) for i in range(mine.shape[0])
    ]


def piece_sum(*parts):
    return summed(jnp.stack(parts))


def input_sum(*parts):
    acc = parts[0].astype(F32)
    for part in parts[1:]:
        acc = acc + part.astype(F32)
    return acc.astype(BF16)


def piece_sum(*parts):
    acc = parts[0]
    for part in parts[1:]:
        acc = acc + part
    return acc


def square_sum(parts):
    return jnp.sum(parts[:, 0, :], axis=0, keepdims=True)


def exchange(parts, axis):
    return lax.all_to_all(parts, axis, split_axis=0, concat_axis=0, tiled=True)


def around(parts, axis, step):
    count = lax.axis_size(axis)
    ring = count // step
    got = [parts[0]]
    for d in range(1, ring):
        route = [(i, (i + d * step) % count) for i in range(count)]
        got.append(lax.ppermute(parts[d], axis, route))
    return got


def per_device(
    block_source,
    address_weights,
    causal_filter_taps,
    payload_vectors,
    probe_vectors,
    interval_preimage,
    channel_damping_exponent,
    added_damping_jumps,
    sigmoid_argument,
    adjoint_of_result,
):
    return step(
        block_source,
        address_weights,
        causal_filter_taps,
        payload_vectors,
        probe_vectors,
        interval_preimage.T,
        channel_damping_exponent.reshape(R, 1),
        added_damping_jumps.T,
        sigmoid_argument,
        adjoint_of_result,
    )


def step(x, w, taps, v, q, tpre, aexp, jump, gate, adj):
    zs = lax.axis_size("z")
    sp = zs * Y
    tp = lax.axis_size("tp")
    features = x.shape[1]
    width = features // zs
    small = (tpre, aexp, jump, gate, adj)
    bwd_send = local(bwd_local, sds((Y, NS + PAD, HP), BF16), *small, q)
    got = exchange(bwd_send, "y")
    rim = lax.ppermute(x[TOK - PAD :], ZY, [(i, i + 1) for i in range(sp - 1)])
    xs = around([x] * Y, "y", 1)
    rows = TOK + 8 * PAD + 2 * NS
    *mids, keys = local(
        fwd_local,
        [sds((rows, HP), BF16)] * Y + [sds((STATE, TOK), BF16)],
        *small,
        q,
        v,
        x,
        w,
        rim,
        taps,
    )
    mids = around(mids, "y", 1)
    bwd_totals = local(bwd_group, sds((zs, NS + PAD, HP), BF16), got)
    far = exchange(bwd_totals, "z")
    near_send, ends, main, over = local(
        bwd_apply,
        [
            sds((zs, NS, width + HP), BF16),
            sds((Y, NS, HP), BF16),
            sds((NS, Y * TOK), F32),
            sds((NS, TOK), F32),
        ],
        far,
        got,
        *mids,
        *xs,
        taps,
    )
    near = exchange(near_send, "z")
    after = lax.ppermute(over, "z", [(i, i - 1) for i in range(1, zs)])
    tokens = local(own_tokens, [sds((NS, TOK), BF16)] * Y, main, after)
    tokens = around(tokens, "y", 1)
    chips = tp // CORES
    share = (features // tp, TOK)
    sides = local(partial_input, [sds((chips, *share), BF16)] * CORES, w, *tokens, raw=(0,))
    swap = [(i, i ^ 1) for i in range(tp)]
    other = lax.ppermute(sides[-1], "tp", swap) if CORES > 1 else None
    *pieces, squares = local(
        weight_sum, [sds((width // Y, STATE), F32)] * Y + [sds((sp, 1, STATE), F32)], near
    )
    squares = exchange(squares, ZY)
    states = local(fwd_apply, [sds((2 * NS, HP), BF16)] * Y, near, far, got, *mids, ends)
    states = around(states, "y", 1)
    if CORES > 1:
        shares = local(core_sum, [sds(share, BF16)] * chips, sides[0], other)
    else:
        shares = [sides[0][i] for i in range(chips)]
    shares = around(shares, "tp", CORES)
    pieces = around(pieces, "y", 1)
    value_grad, query_grad, decay_grad, gate_grad = local(
        finish,
        [sds((TOK, HP), BF16), sds((TOK, STATE), BF16), sds((R, TOK), F32), sds((TOK, HP), BF16)],
        *states,
        *small,
        q,
        v,
        keys,
    )
    input_grad = local(input_sum, sds(share, BF16), *shares)
    key_weight_grad = local(piece_sum, sds((width // Y, STATE), F32), *pieces).T
    row_squares = local(square_sum, sds((1, STATE), F32), squares).reshape(STATE)
    return (
        key_weight_grad,
        row_squares,
        input_grad,
        value_grad,
        query_grad,
        decay_grad.T,
        gate_grad,
    )


def solution(mesh):
    sp, tp = mesh.shape["sp"], mesh.shape["tp"]
    fine = Mesh(mesh.devices.reshape(sp // Y, Y, tp), ("z", "y", "tp"))
    sh = P(ZY, "tp")
    in_specs = (
        P(ZY, None),
        P("tp", None),
        P(None, "tp"),
        sh,
        sh,
        sh,
        P("tp"),
        sh,
        sh,
        sh,
    )
    out_specs = (P("tp", ZY), P("tp"), P("tp", ZY), sh, sh, sh, sh)
    return jax.shard_map(
        per_device, mesh=fine, in_specs=in_specs, out_specs=out_specs, check_vma=False
    )
```

```python
import jax
import jax.numpy as jnp
from jax import lax
from jax.experimental import pallas as pl
from jax.experimental.pallas import tpu as pltpu
from jax.sharding import Mesh
from jax.sharding import PartitionSpec as P


TOK = 128
STATE = 128
HEAD = 64
R = 4
HP = R * HEAD
Y = 4
NS = STATE // Y
PAD = 8
HIGH = lax.Precision.HIGHEST
F32 = jnp.float32
BF16 = jnp.bfloat16
PALLAS = True
ZY = ("z", "y")
VMEM_LIMIT = 16 * 2**20
BIG = 60 * 1024 * 2**10


def dot(a, b, ca=1, cb=0, precision=None):
    return lax.dot_general(
        a, b, (((ca,), (cb,)), ((), ())), preferred_element_type=F32, precision=precision
    )


def roll(a, shift):
    size = a.shape[1]
    if PALLAS:
        return pltpu.roll(a, shift % size, 1)
    return jnp.roll(a, shift, axis=1)


def local(fn, outs, *args, flops=10**7, raw=(), vmem=VMEM_LIMIT):
    single = not isinstance(outs, (list, tuple))
    shapes = [outs] if single else list(outs)
    if not PALLAS:
        res = fn(*args)
        res = [res] if single else list(res)
        for r, s in zip(res, shapes):
            assert r.shape == s.shape and r.dtype == s.dtype, (fn, r, s)
        return res[0] if single else res

    def kernel(*refs):
        ins, dst = refs[: len(args)], refs[len(args) :]
        res = fn(*[r if i in raw else r[...] for i, r in enumerate(ins)])
        res = [res] if single else res
        for ref, val in zip(dst, res):
            ref[...] = val

    vm = pl.BlockSpec(memory_space=pltpu.VMEM)
    res = pl.pallas_call(
        kernel,
        out_shape=shapes,
        in_specs=[vm] * len(args),
        out_specs=[vm] * len(shapes),
        cost_estimate=pl.CostEstimate(flops=flops, bytes_accessed=10**6, transcendentals=0),
        compiler_params=pltpu.CompilerParams(vmem_limit_bytes=vmem),
    )(*args)
    return res[0] if single else res


def sds(shape, dtype):
    return jax.ShapeDtypeStruct(shape, dtype)


def choose(parts, index):
    res = parts[0]
    for i in range(1, len(parts)):
        res = jnp.where(index == i, parts[i], res)
    return res


def to_peers(parts):
    yi = lax.axis_index("y")
    return [choose(parts, lax.rem(yi + d, Y)) for d in range(Y)]


def from_peers(parts):
    yi = lax.axis_index("y")
    return [choose(parts, lax.rem(yi + Y - j, Y)) for j in range(Y)]


def by_mask(parts):
    yi = lax.axis_index("y")
    return [choose(parts, jnp.bitwise_xor(yi, j)) for j in range(Y)]


def columns_at(ref, start, size):
    if PALLAS:
        return ref[:, pl.ds(pl.multiple_of(start, size), size)]
    return lax.dynamic_slice_in_dim(ref, start, size, axis=1)


def iota2(shape, dim):
    return lax.broadcasted_iota(jnp.int32, shape, dim)


def expand(a):
    return jnp.concatenate(
        [jnp.broadcast_to(a[:, h : h + 1], (a.shape[0], HEAD)) for h in range(R)], axis=1
    )


def split3(a):
    hi = a.astype(BF16)
    rest = a - hi.astype(F32)
    mid = rest.astype(BF16)
    low = (rest - mid.astype(F32)).astype(BF16)
    return hi, mid, low


def joined(parts, first):
    return (
        parts[:, first].astype(F32)
        + parts[:, first + 1].astype(F32)
        + parts[:, first + 2].astype(F32)
    )


def column(a):
    eye = (iota2((TOK, TOK), 0) == iota2((TOK, TOK), 1)).astype(F32)
    return dot(eye, a, 1, 1, HIGH)


def decays(tpre, aexp, jump):
    step = jnp.log(1.0 + jnp.exp(tpre))
    same = iota2((R, R), 0) == iota2((R, R), 1)
    rate = jnp.sum(jnp.where(same, jnp.exp(aexp), 0.0), axis=1, keepdims=True)
    la = jump - rate * step
    tri = (iota2((TOK, TOK), 0) >= iota2((TOK, TOK), 1)).astype(F32)
    cum = dot(tri, la, 1, 1, HIGH)
    return step, rate, la, cum


def row_form(la):
    upper = (iota2((TOK, TOK), 0) <= iota2((TOK, TOK), 1)).astype(F32)
    return dot(la, upper, precision=HIGH)


def sigmoid(v):
    return 1.0 / (1.0 + jnp.exp(-v))


def bwd_local(tpre, aexp, jump, gate, adj, q, v):
    step, _, _, cum = decays(tpre, aexp, jump)
    g = gate.astype(F32)
    dy = adj.astype(F32) * g * sigmoid(g)
    dye = (dy * expand(jnp.exp(cum))).astype(BF16)
    lg = dot(q, dye, 0, 0).astype(BF16)
    ud = v.astype(F32) * expand(column(step) * jnp.exp(cum[TOK - 1 :] - cum))
    hi, mid, low = split3(expand(cum[TOK - 1 :]))
    tail = jnp.concatenate(
        [hi, mid, low, jnp.zeros((PAD - 3, HP), BF16), ud.astype(BF16)], axis=0
    )
    return jnp.stack([jnp.concatenate([lg[NS * i : NS * (i + 1)], tail], axis=0) for i in range(Y)])


def masks_of(cum, cum_t, h):
    causal = iota2((TOK, TOK), 0) >= iota2((TOK, TOK), 1)
    return jnp.exp(jnp.where(causal, cum[:, h : h + 1] - cum_t[h : h + 1, :], -1e30))


def fwd_local(tpre, aexp, jump, gate, adj, q, v, x, w, rim, taps):
    step, _, la, cum = decays(tpre, aexp, jump)
    cum_t = row_form(la)
    taps_t = column(taps)
    rim = jnp.where(iota2(rim.shape, 0) >= PAD - 3, rim.astype(F32), 0.0).astype(BF16)
    g = gate.astype(F32)
    dy = (adj.astype(F32) * g * sigmoid(g)).astype(BF16)
    u = v.astype(F32) * expand(column(step))
    ud = (u * expand(jnp.exp(cum[TOK - 1 :] - cum))).astype(BF16)
    u = u.astype(BF16)
    dc = jnp.zeros((TOK, TOK), F32)
    for h in range(R):
        at = slice(HEAD * h, HEAD * (h + 1))
        dc = dc + masks_of(cum, cum_t, h) * dot(dy[:, at], u[:, at], 1, 1)
    dki = dot(q, dc.astype(BF16), 0, 0)
    proj = dot(w, x, 1, 1).astype(BF16).astype(F32)
    rim_proj = dot(w, rim, 1, 1).astype(BF16)
    place = (iota2((PAD, TOK), 1) == iota2((PAD, TOK), 0) + (TOK - PAD)).astype(BF16)
    rim_full = dot(rim_proj, place)
    lane = iota2((STATE, TOK), 1)
    conv = taps_t[:, 3:4] * proj
    for d in range(1, 4):
        conv = conv + taps_t[:, 3 - d : 4 - d] * roll(
            jnp.where(lane >= TOK - d, rim_full, proj), d
        )
    sig = sigmoid(conv)
    keys = (conv * sig).astype(BF16)
    slope = sig * (1.0 + conv * (1.0 - sig))
    ls = dot(keys, ud).astype(BF16)
    pair = jnp.concatenate([dki.astype(BF16), slope.astype(BF16)], axis=1)
    eye = (iota2((TOK, TOK), 0) == iota2((TOK, TOK), 1)).astype(BF16)
    xt = dot(x, eye, 0, 0).astype(BF16)
    small_eye = (iota2((PAD, PAD), 0) == iota2((PAD, PAD), 1)).astype(BF16)
    rt = dot(rim, small_eye, 0, 0).astype(BF16)
    width = Y * NS
    blocks = x.shape[1] // width

    def features_of(a, i):
        return jnp.concatenate(
            [a[width * b + NS * i : width * b + NS * (i + 1)] for b in range(blocks)], axis=0
        )

    mids = []
    for i in range(Y):
        xs = features_of(xt, i)
        rs = dot(small_eye, features_of(rt, i), 1, 1).astype(BF16)
        half = xs.shape[0] // 2
        mids.append(
            jnp.concatenate(
                [
                    pair,
                    ls[NS * i : NS * (i + 1)],
                    jnp.concatenate([xs[:half], xs[half:]], axis=1),
                    rs[:, :half],
                    rs[:, half:],
                ],
                axis=0,
            )
        )
    return *to_peers(mids), keys


def bwd_group(got):
    tau = joined(got, NS)
    acc = got[Y - 1, :NS].astype(F32)
    for j in range(Y - 2, -1, -1):
        acc = got[j, :NS].astype(F32) + jnp.exp(tau[j : j + 1]) * acc
    hi, mid, low = split3(jnp.sum(tau, axis=0, keepdims=True))
    part = jnp.concatenate(
        [acc.astype(BF16), hi, mid, low, jnp.zeros((PAD - 3, HP), BF16)], axis=0
    )
    return jnp.stack([part] * lax.axis_size("z"))


def fwd_group(got, mid):
    tau = joined(got, NS)
    at = slice(TOK, TOK + NS)
    acc = mid[0][at].astype(F32)
    for j in range(1, Y):
        acc = mid[j][at].astype(F32) + jnp.exp(tau[j : j + 1]) * acc
    return acc.astype(BF16)


def chain_sums(far):
    count = far.shape[0]
    tau = joined(far, NS)
    tri = (iota2((count, count), 0) >= iota2((count, count), 1)).astype(F32)
    upto = dot(tri, tau, precision=HIGH)
    return tau, upto


def weighted(weights, far):
    acc = weights[0:1] * far[0, :NS].astype(F32)
    for i in range(1, far.shape[0]):
        acc = acc + weights[i : i + 1] * far[i, :NS].astype(F32)
    return acc


def bwd_far(far, got):
    count = far.shape[0]
    zrow = lax.axis_index("z")
    tau, upto = chain_sums(far)
    row = iota2((count, HP), 0)
    mine = jnp.sum(jnp.where(row == zrow, upto, 0.0), axis=0, keepdims=True)
    weights = jnp.exp(jnp.where(row > zrow, upto - tau - mine, -1e30))
    state = weighted(weights, far)
    tau_j = joined(got, NS)
    ends = [None] * Y
    for j in range(Y - 1, -1, -1):
        ends[j] = state.astype(BF16)
        if j:
            state = got[j, :NS].astype(F32) + jnp.exp(tau_j[j : j + 1]) * state
    dk = [dot(ends[j], got[j, NS + PAD :], 1, 1).astype(BF16) for j in range(Y)]
    halves = [jnp.concatenate(dk[i : i + 2], axis=1) for i in range(0, Y, 2)]
    return jnp.stack([jnp.concatenate([*halves, ends[j]], axis=0) for j in range(Y)])


def key_grads(near, got, m0, m1, m2, m3, taps):
    mid = from_peers([m0, m1, m2, m3])
    yi = lax.axis_index("y")
    taps_t = column(taps)
    dk = jnp.concatenate(
        [
            jnp.concatenate([near[i, :NS], near[i, NS : 2 * NS]], axis=1).astype(F32)
            for i in range(Y)
        ],
        axis=0,
    )
    dki = jnp.concatenate([part[:STATE, :TOK] for part in mid], axis=1).astype(F32)
    slope = jnp.concatenate([part[:STATE, TOK:] for part in mid], axis=1).astype(F32)
    cg = (dk + dki) * slope
    size = Y * TOK
    lane = iota2((STATE, size), 1)
    main = taps_t[:, 3:4] * cg
    over = jnp.zeros_like(main)
    for d in range(1, 4):
        moved = taps_t[:, 3 - d : 4 - d] * roll(cg, -d)
        main = main + jnp.where(lane < size - d, moved, 0.0)
        over = over + jnp.where(lane >= size - d, moved, 0.0)
    over = over[:, size - TOK :]
    pg = main.astype(BF16)
    first = TOK + NS
    last = mid[0].shape[0] - 2 * PAD
    rims = jnp.concatenate([mid[0][last : last + PAD], mid[0][last + PAD :]], axis=1)
    dw = dot(rims, over[:, TOK - PAD :].astype(BF16), 0, 1)
    for j in range(Y):
        xs = jnp.concatenate([mid[j][first:last, :TOK], mid[j][first:last, TOK:]], axis=0)
        dw = dw + dot(xs, pg[:, TOK * j : TOK * (j + 1)], 1, 1)
    dw = dw.astype(BF16)
    fwd = fwd_group(got, mid)
    send = jnp.stack(
        [
            jnp.concatenate([dw[NS * i : NS * (i + 1)], fwd], axis=1)
            for i in range(dw.shape[0] // NS)
        ]
    )
    own = choose([main[:, TOK * j : TOK * (j + 1)] for j in range(Y)], yi)
    return send, own, over


def fwd_apply(near, bfar, got, m0, m1, m2, m3):
    mid = from_peers([m0, m1, m2, m3])
    far = near[:, :, near.shape[2] - HP :]
    zrow = lax.axis_index("z")
    count = far.shape[0]
    tau, upto = chain_sums(bfar)
    row = iota2((count, HP), 0)
    before = jnp.sum(jnp.where(row == zrow, upto - tau, 0.0), axis=0, keepdims=True)
    weights = jnp.exp(jnp.where(row < zrow, before - upto, -1e30))
    state = weighted(weights, far)
    tau_j = joined(got, NS)
    at = slice(TOK, TOK + NS)
    res = []
    for j in range(Y):
        res.append(state.astype(BF16))
        if j < Y - 1:
            state = mid[j][at].astype(F32) + jnp.exp(tau_j[j : j + 1]) * state
    mine, one, two, three = by_mask(res)
    return mine, jnp.concatenate([one, two], axis=0), three


def finish(mine, first, second, near, tpre, aexp, jump, gate, adj, q, v, keys):
    step, rate, la, cum = decays(tpre, aexp, jump)
    cum_t = row_form(la)
    s_in = jnp.concatenate(by_mask([mine, first[:NS], second[NS:], second[:NS]]), axis=0)
    g_out = jnp.concatenate([near[i, 2 * NS :] for i in range(Y)], axis=0)
    g = gate.astype(F32)
    a = adj.astype(F32)
    sig = sigmoid(g)
    dy = a * g * sig
    vw = v.astype(F32)
    stepw = expand(column(step))
    u = vw * stepw
    e = expand(jnp.exp(cum))
    d = expand(jnp.exp(cum[TOK - 1 :] - cum))
    dyb, ub = dy.astype(BF16), u.astype(BF16)
    scores = dot(q, keys)
    y_far = e * dot(q, s_in)
    du_far = d * dot(keys, g_out, 0, 0)
    dc = jnp.zeros((TOK, TOK), F32)
    ys, dus, diffs = [], [], []
    for h in range(R):
        at = slice(HEAD * h, HEAD * (h + 1))
        mask = masks_of(cum, cum_t, h)
        z = dot(dyb[:, at], ub[:, at], 1, 1)
        lz = mask * z
        dc = dc + lz
        m = lz * scores
        diffs.append(jnp.sum(m.T - m, axis=0, keepdims=True))
        lc = (mask * scores).astype(BF16)
        ys.append(dot(lc, ub[:, at]))
        dus.append(dot(lc, dyb[:, at], 0, 0))
    y = y_far + jnp.concatenate(ys, axis=1)
    du = du_far + jnp.concatenate(dus, axis=1)
    pick = (iota2((R, HP), 1) // HEAD == iota2((R, HP), 0)).astype(F32)
    from_d = dot(pick, u * du_far, 1, 1, HIGH)
    dcum = jnp.concatenate(diffs, axis=0) + dot(pick, dy * y_far, 1, 1, HIGH) - from_d
    kept = jnp.sum(s_in.astype(F32) * g_out.astype(F32), axis=0, keepdims=True)
    kept = kept * expand(jnp.exp(cum[TOK - 1 :]))
    dtot = jnp.sum(from_d, axis=1, keepdims=True) + jnp.sum(pick * kept, axis=1, keepdims=True)
    later = (iota2((TOK, TOK), 0) >= iota2((TOK, TOK), 1)).astype(F32)
    dla = dot(dcum, later, precision=HIGH) + dtot
    dstep = dot(pick, du * vw, 1, 1, HIGH) - rate * dla
    decay_grad = dstep * sigmoid(tpre)
    value_grad = (du * stepw).astype(BF16)
    query_grad = (
        dot(dc.astype(BF16), keys, 1, 1) + dot((dy * e).astype(BF16), s_in, 1, 1)
    ).astype(BF16)
    gate_grad = (a * y * (sig * (1.0 + g * (1.0 - sig)))).astype(BF16)
    return value_grad, query_grad, decay_grad, gate_grad


def summed(parts):
    acc = parts[0].astype(F32)
    for i in range(1, parts.shape[0]):
        acc = acc + parts[i].astype(F32)
    return acc


def weight_sum(near):
    acc = summed(near[:, :, :STATE])
    count = lax.axis_size("z") * Y
    squares = jnp.sum(acc * acc, axis=0, keepdims=True)
    return acc, jnp.broadcast_to(squares[None], (count, 1, STATE))


def partial_input(w, own, after):
    edge = lax.axis_index("y") == Y - 1
    grad = (own + jnp.where(edge, after, 0.0)).astype(BF16)
    place = lax.axis_index("tp")
    width = w.shape[1] // lax.axis_size("tp")
    core = lax.rem(place, 2)
    chip = lax.div(place, 2)
    near = jnp.bitwise_xor(chip, 1)
    chips = (chip, 3 - chip, near, 3 - near)
    res = []
    for owner in (core, 1 - core):
        blocks = []
        for other in chips:
            rank = other * 2 + owner
            blocks.append(dot(columns_at(w, rank * width, width), grad, 0, 0).astype(BF16))
        res.append(jnp.stack(blocks))
    return res


def half_sum(mine, other):
    size = mine.shape[0] // 2
    total = (mine.astype(F32) + other.astype(F32)).astype(BF16)
    return total[:size], total[size:]


def last_sum(mine, other):
    return (mine[0].astype(F32) + other[0].astype(F32)).astype(BF16)


def square_sum(parts):
    return jnp.sum(parts[:, 0, :], axis=0, keepdims=True)


def exchange(parts, axis):
    return lax.all_to_all(parts, axis, split_axis=0, concat_axis=0, tiled=True)


def around(parts, axis, step):
    count = lax.axis_size(axis)
    ring = count // step
    got = [parts[0]]
    for d in range(1, ring):
        route = [(i, (i + d * step) % count) for i in range(count)]
        got.append(lax.ppermute(parts[d], axis, route))
    return got


def per_device(
    block_source,
    address_weights,
    causal_filter_taps,
    payload_vectors,
    probe_vectors,
    interval_preimage,
    channel_damping_exponent,
    added_damping_jumps,
    sigmoid_argument,
    adjoint_of_result,
):
    return step(
        block_source,
        address_weights,
        causal_filter_taps,
        payload_vectors,
        probe_vectors,
        interval_preimage.T,
        channel_damping_exponent.reshape(1, R),
        added_damping_jumps.T,
        sigmoid_argument,
        adjoint_of_result,
    )


def step(x, w, taps, v, q, tpre, aexp, jump, gate, adj):
    zs = lax.axis_size("z")
    sp = zs * Y
    tp = lax.axis_size("tp")
    features = x.shape[1]
    small = (tpre, aexp, jump, gate, adj)
    bwd_send = local(bwd_local, sds((Y, NS + PAD + TOK, HP), BF16), *small, q, v, vmem=BIG)
    got = exchange(bwd_send, "y")
    rim = lax.ppermute(x[TOK - PAD :], ZY, [(i, i + 1) for i in range(sp - 1)])
    rows = TOK + NS + features // Y // 2 + 2 * PAD
    *mids, keys = local(
        fwd_local,
        [sds((rows, HP), BF16)] * Y + [sds((STATE, TOK), BF16)],
        *small,
        q,
        v,
        x,
        w,
        rim,
        taps,
    )
    mids = around(mids, "y", 1)
    bwd_totals = local(bwd_group, sds((zs, NS + PAD, HP), BF16), got)
    far = exchange(bwd_totals, "z")
    ends = local(bwd_far, sds((Y, 3 * NS, HP), BF16), far, got)
    ends = exchange(ends, "y")
    send, own, over = local(
        key_grads,
        [sds((zs, NS, STATE + HP), BF16), sds((STATE, TOK), F32), sds((STATE, TOK), F32)],
        ends,
        got,
        *mids,
        taps,
    )
    near = exchange(send, "z")
    after = lax.ppermute(over, "z", [(i, i - 1) for i in range(1, zs)])
    weight_t, squares = local(
        weight_sum, [sds((NS, STATE), F32), sds((sp, 1, STATE), F32)], near
    )
    squares = exchange(squares, ZY)
    mine, first, second = local(
        fwd_apply,
        [sds((NS, HP), BF16), sds((2 * NS, HP), BF16), sds((NS, HP), BF16)],
        near,
        far,
        got,
        *mids,
    )
    first = lax.ppermute(first, "y", [(i, i ^ 1) for i in range(Y)])
    second = jnp.concatenate([second, first[NS:]], axis=0)
    second = lax.ppermute(second, "y", [(i, i ^ 3) for i in range(Y)])
    share = (features // tp, TOK)
    keep, give = local(partial_input, [sds((4, *share), BF16)] * 2, w, own, after, raw=(0,))
    give = lax.ppermute(give, "tp", [(i, i ^ 1) for i in range(tp)])
    keep, give = local(half_sum, [sds((2, *share), BF16)] * 2, keep, give)
    give = lax.ppermute(give, "tp", [(i, i ^ 2) for i in range(tp)])
    keep, give = local(half_sum, [sds((1, *share), BF16)] * 2, keep, give)
    give = lax.ppermute(give, "tp", [(i, i ^ 6) for i in range(tp)])
    input_grad = local(last_sum, sds(share, BF16), keep, give)
    value_grad, query_grad, decay_grad, gate_grad = local(
        finish,
        [sds((TOK, HP), BF16), sds((TOK, STATE), BF16), sds((R, TOK), F32), sds((TOK, HP), BF16)],
        mine,
        first,
        second,
        ends,
        *small,
        q,
        v,
        keys,
    )
    row_squares = local(square_sum, sds((1, STATE), F32), squares).reshape(STATE)
    return (
        weight_t.T,
        row_squares,
        input_grad,
        value_grad,
        query_grad,
        decay_grad.T,
        gate_grad,
    )


def solution(mesh):
    sp, tp = mesh.shape["sp"], mesh.shape["tp"]
    fine = Mesh(mesh.devices.reshape(sp // Y, Y, tp), ("z", "y", "tp"))
    sh = P(ZY, "tp")
    in_specs = (
        P(ZY, None),
        P("tp", None),
        P(None, "tp"),
        sh,
        sh,
        sh,
        P("tp"),
        sh,
        sh,
        sh,
    )
    out_specs = (P("tp", ZY), P("tp"), P("tp", ZY), sh, sh, sh, sh)
    return jax.shard_map(
        per_device, mesh=fine, in_specs=in_specs, out_specs=out_specs, check_vma=False
    )
```

```python
import jax
import jax.numpy as jnp
from jax import lax
from jax.experimental import pallas as pl
from jax.experimental.pallas import tpu as pltpu
from jax.sharding import Mesh
from jax.sharding import PartitionSpec as P


TOK = 128
STATE = 128
HEAD = 64
R = 4
HP = R * HEAD
Y = 4
NS = STATE // Y
PAD = 8
HIGH = lax.Precision.HIGHEST
F32 = jnp.float32
BF16 = jnp.bfloat16
PALLAS = True
ZY = ("z", "y")
VMEM_LIMIT = 16 * 2**20
BIG = 60 * 1024 * 2**10


def dot(a, b, ca=1, cb=0, precision=None):
    return lax.dot_general(
        a, b, (((ca,), (cb,)), ((), ())), preferred_element_type=F32, precision=precision
    )


def roll(a, shift):
    size = a.shape[1]
    if PALLAS:
        return pltpu.roll(a, shift % size, 1)
    return jnp.roll(a, shift, axis=1)


def local(fn, outs, *args, flops=10**7, raw=(), vmem=VMEM_LIMIT):
    single = not isinstance(outs, (list, tuple))
    shapes = [outs] if single else list(outs)
    if not PALLAS:
        res = fn(*args)
        res = [res] if single else list(res)
        for r, s in zip(res, shapes):
            assert r.shape == s.shape and r.dtype == s.dtype, (fn, r, s)
        return res[0] if single else res

    def kernel(*refs):
        ins, dst = refs[: len(args)], refs[len(args) :]
        res = fn(*[r if i in raw else r[...] for i, r in enumerate(ins)])
        res = [res] if single else res
        for ref, val in zip(dst, res):
            ref[...] = val

    vm = pl.BlockSpec(memory_space=pltpu.VMEM)
    res = pl.pallas_call(
        kernel,
        out_shape=shapes,
        in_specs=[vm] * len(args),
        out_specs=[vm] * len(shapes),
        cost_estimate=pl.CostEstimate(flops=flops, bytes_accessed=10**6, transcendentals=0),
        compiler_params=pltpu.CompilerParams(vmem_limit_bytes=vmem),
    )(*args)
    return res[0] if single else res


def sds(shape, dtype):
    return jax.ShapeDtypeStruct(shape, dtype)


def choose(parts, index):
    res = parts[0]
    for i in range(1, len(parts)):
        res = jnp.where(index == i, parts[i], res)
    return res


def to_peers(parts):
    yi = lax.axis_index("y")
    return [choose(parts, lax.rem(yi + d, Y)) for d in range(Y)]


def from_peers(parts):
    yi = lax.axis_index("y")
    return [choose(parts, lax.rem(yi + Y - j, Y)) for j in range(Y)]


def columns_at(ref, start, size):
    if PALLAS:
        return ref[:, pl.ds(pl.multiple_of(start, size), size)]
    return lax.dynamic_slice_in_dim(ref, start, size, axis=1)


def iota2(shape, dim):
    return lax.broadcasted_iota(jnp.int32, shape, dim)


def expand(a):
    return jnp.concatenate(
        [jnp.broadcast_to(a[:, h : h + 1], (a.shape[0], HEAD)) for h in range(R)], axis=1
    )


def split3(a):
    hi = a.astype(BF16)
    rest = a - hi.astype(F32)
    mid = rest.astype(BF16)
    low = (rest - mid.astype(F32)).astype(BF16)
    return hi, mid, low


def joined(parts, first):
    return (
        parts[:, first].astype(F32)
        + parts[:, first + 1].astype(F32)
        + parts[:, first + 2].astype(F32)
    )


def column(a):
    eye = (iota2((TOK, TOK), 0) == iota2((TOK, TOK), 1)).astype(F32)
    return dot(eye, a, 1, 1, HIGH)


def decays(tpre, aexp, jump):
    step = jnp.log(1.0 + jnp.exp(tpre))
    same = iota2((R, R), 0) == iota2((R, R), 1)
    rate = jnp.sum(jnp.where(same, jnp.exp(aexp), 0.0), axis=1, keepdims=True)
    la = jump - rate * step
    tri = (iota2((TOK, TOK), 0) >= iota2((TOK, TOK), 1)).astype(F32)
    cum = dot(tri, la, 1, 1, HIGH)
    return step, rate, la, cum


def row_form(la):
    upper = (iota2((TOK, TOK), 0) <= iota2((TOK, TOK), 1)).astype(F32)
    return dot(la, upper, precision=HIGH)


def sigmoid(v):
    return 1.0 / (1.0 + jnp.exp(-v))


def bwd_local(tpre, aexp, jump, gate, adj, q, v):
    step, _, _, cum = decays(tpre, aexp, jump)
    g = gate.astype(F32)
    dy = adj.astype(F32) * g * sigmoid(g)
    dye = (dy * expand(jnp.exp(cum))).astype(BF16)
    lg = dot(q, dye, 0, 0).astype(BF16)
    ud = v.astype(F32) * expand(column(step) * jnp.exp(cum[TOK - 1 :] - cum))
    hi, mid, low = split3(expand(cum[TOK - 1 :]))
    tail = jnp.concatenate(
        [hi, mid, low, jnp.zeros((PAD - 3, HP), BF16), ud.astype(BF16)], axis=0
    )
    return jnp.stack([jnp.concatenate([lg[NS * i : NS * (i + 1)], tail], axis=0) for i in range(Y)])


def masks_of(cum, cum_t, h):
    causal = iota2((TOK, TOK), 0) >= iota2((TOK, TOK), 1)
    return jnp.exp(jnp.where(causal, cum[:, h : h + 1] - cum_t[h : h + 1, :], -1e30))


def fwd_local(tpre, aexp, jump, gate, adj, q, v, x, w, rim, taps):
    step, _, la, cum = decays(tpre, aexp, jump)
    cum_t = row_form(la)
    taps_t = column(taps)
    rim = jnp.where(iota2(rim.shape, 0) >= PAD - 3, rim.astype(F32), 0.0).astype(BF16)
    g = gate.astype(F32)
    dy = (adj.astype(F32) * g * sigmoid(g)).astype(BF16)
    u = v.astype(F32) * expand(column(step))
    ud = (u * expand(jnp.exp(cum[TOK - 1 :] - cum))).astype(BF16)
    u = u.astype(BF16)
    dc = jnp.zeros((TOK, TOK), F32)
    for h in range(R):
        at = slice(HEAD * h, HEAD * (h + 1))
        dc = dc + masks_of(cum, cum_t, h) * dot(dy[:, at], u[:, at], 1, 1)
    dki = dot(q, dc.astype(BF16), 0, 0)
    proj = dot(w, x, 1, 1).astype(BF16).astype(F32)
    rim_proj = dot(w, rim, 1, 1).astype(BF16)
    place = (iota2((PAD, TOK), 1) == iota2((PAD, TOK), 0) + (TOK - PAD)).astype(BF16)
    rim_full = dot(rim_proj, place)
    lane = iota2((STATE, TOK), 1)
    conv = taps_t[:, 3:4] * proj
    for d in range(1, 4):
        conv = conv + taps_t[:, 3 - d : 4 - d] * roll(
            jnp.where(lane >= TOK - d, rim_full, proj), d
        )
    sig = sigmoid(conv)
    keys = (conv * sig).astype(BF16)
    slope = sig * (1.0 + conv * (1.0 - sig))
    ls = dot(keys, ud).astype(BF16)
    pair = jnp.concatenate([dki.astype(BF16), slope.astype(BF16)], axis=1)
    eye = (iota2((TOK, TOK), 0) == iota2((TOK, TOK), 1)).astype(BF16)
    xt = dot(x, eye, 0, 0).astype(BF16)
    small_eye = (iota2((PAD, PAD), 0) == iota2((PAD, PAD), 1)).astype(BF16)
    rt = dot(rim, small_eye, 0, 0).astype(BF16)
    width = Y * NS
    blocks = x.shape[1] // width

    def features_of(a, i):
        return jnp.concatenate(
            [a[width * b + NS * i : width * b + NS * (i + 1)] for b in range(blocks)], axis=0
        )

    mids = []
    for i in range(Y):
        xs = features_of(xt, i)
        rs = dot(small_eye, features_of(rt, i), 1, 1).astype(BF16)
        half = xs.shape[0] // 2
        mids.append(
            jnp.concatenate(
                [
                    pair,
                    ls[NS * i : NS * (i + 1)],
                    jnp.concatenate([xs[:half], xs[half:]], axis=1),
                    rs[:, :half],
                    rs[:, half:],
                ],
                axis=0,
            )
        )
    return *to_peers(mids), keys


def bwd_group(got):
    tau = joined(got, NS)
    acc = got[Y - 1, :NS].astype(F32)
    for j in range(Y - 2, -1, -1):
        acc = got[j, :NS].astype(F32) + jnp.exp(tau[j : j + 1]) * acc
    hi, mid, low = split3(jnp.sum(tau, axis=0, keepdims=True))
    part = jnp.concatenate(
        [acc.astype(BF16), hi, mid, low, jnp.zeros((PAD - 3, HP), BF16)], axis=0
    )
    return jnp.stack([part] * lax.axis_size("z"))


def fwd_group(got, mid):
    tau = joined(got, NS)
    at = slice(TOK, TOK + NS)
    acc = mid[0][at].astype(F32)
    for j in range(1, Y):
        acc = mid[j][at].astype(F32) + jnp.exp(tau[j : j + 1]) * acc
    return acc.astype(BF16)


def chain_sums(far):
    count = far.shape[0]
    tau = joined(far, NS)
    tri = (iota2((count, count), 0) >= iota2((count, count), 1)).astype(F32)
    upto = dot(tri, tau, precision=HIGH)
    return tau, upto


def weighted(weights, far):
    acc = weights[0:1] * far[0, :NS].astype(F32)
    for i in range(1, far.shape[0]):
        acc = acc + weights[i : i + 1] * far[i, :NS].astype(F32)
    return acc


def bwd_far(far, got, m0, m1, m2, m3):
    mid = from_peers([m0, m1, m2, m3])
    count = far.shape[0]
    zrow = lax.axis_index("z")
    tau, upto = chain_sums(far)
    row = iota2((count, HP), 0)
    mine = jnp.sum(jnp.where(row == zrow, upto, 0.0), axis=0, keepdims=True)
    weights = jnp.exp(jnp.where(row > zrow, upto - tau - mine, -1e30))
    state = weighted(weights, far)
    tau_j = joined(got, NS)
    ends = [None] * Y
    for j in range(Y - 1, -1, -1):
        ends[j] = state.astype(BF16)
        if j:
            state = got[j, :NS].astype(F32) + jnp.exp(tau_j[j : j + 1]) * state
    dk = [dot(ends[j], got[j, NS + PAD :], 1, 1).astype(BF16) for j in range(Y)]
    halves = [jnp.concatenate(dk[i : i + 2], axis=1) for i in range(0, Y, 2)]
    begins = [jnp.zeros((NS, HP), F32)]
    for j in range(Y - 1):
        begins.append(
            mid[j][TOK : TOK + NS].astype(F32) + jnp.exp(tau_j[j : j + 1]) * begins[j]
        )
    return jnp.stack(
        [
            jnp.concatenate([*halves, ends[j], begins[j].astype(BF16)], axis=0)
            for j in range(Y)
        ]
    )


def key_grads(near, got, m0, m1, m2, m3, taps):
    mid = from_peers([m0, m1, m2, m3])
    yi = lax.axis_index("y")
    taps_t = column(taps)
    dk = jnp.concatenate(
        [
            jnp.concatenate([near[i, :NS], near[i, NS : 2 * NS]], axis=1).astype(F32)
            for i in range(Y)
        ],
        axis=0,
    )
    dki = jnp.concatenate([part[:STATE, :TOK] for part in mid], axis=1).astype(F32)
    slope = jnp.concatenate([part[:STATE, TOK:] for part in mid], axis=1).astype(F32)
    cg = (dk + dki) * slope
    size = Y * TOK
    lane = iota2((STATE, size), 1)
    main = taps_t[:, 3:4] * cg
    over = jnp.zeros_like(main)
    for d in range(1, 4):
        moved = taps_t[:, 3 - d : 4 - d] * roll(cg, -d)
        main = main + jnp.where(lane < size - d, moved, 0.0)
        over = over + jnp.where(lane >= size - d, moved, 0.0)
    over = over[:, size - TOK :]
    pg = main.astype(BF16)
    first = TOK + NS
    last = mid[0].shape[0] - 2 * PAD
    rims = jnp.concatenate([mid[0][last : last + PAD], mid[0][last + PAD :]], axis=1)
    dw = dot(rims, over[:, TOK - PAD :].astype(BF16), 0, 1)
    for j in range(Y):
        xs = jnp.concatenate([mid[j][first:last, :TOK], mid[j][first:last, TOK:]], axis=0)
        dw = dw + dot(xs, pg[:, TOK * j : TOK * (j + 1)], 1, 1)
    dw = dw.astype(BF16)
    fwd = fwd_group(got, mid)
    count = dw.shape[0] // NS
    each = NS // count
    row, col = iota2((PAD * count, NS), 0), iota2((PAD * count, NS), 1)
    part = lax.rem(row, PAD)
    target = lax.div(row, PAD) * each + lax.rem(part, each)
    tail = jnp.zeros((PAD * count, STATE), F32)
    for half in range(2):
        pick = (col == target) & (lax.div(part, each) == half)
        tail = tail + dot(pick.astype(BF16), fwd[:, STATE * half : STATE * (half + 1)])
    tail = tail.astype(BF16)
    send = jnp.stack(
        [
            jnp.concatenate(
                [dw[NS * i : NS * (i + 1)], tail[PAD * i : PAD * (i + 1)]], axis=0
            )
            for i in range(count)
        ]
    )
    own = choose([main[:, TOK * j : TOK * (j + 1)] for j in range(Y)], yi)
    eye = (iota2((PAD, PAD), 0) == iota2((PAD, PAD), 1)).astype(F32)
    return send, own, dot(eye, over[:, TOK - PAD :], 1, 1, HIGH)


def finish_near(near, got, tpre, aexp, jump, gate, adj, q, v, keys):
    step, rate, la, cum = decays(tpre, aexp, jump)
    cum_t = row_form(la)
    g_out = jnp.concatenate([near[i, 2 * NS : 3 * NS] for i in range(Y)], axis=0)
    g = gate.astype(F32)
    a = adj.astype(F32)
    sig = sigmoid(g)
    dy = a * g * sig
    vw = v.astype(F32)
    stepw = expand(column(step))
    u = vw * stepw
    e = expand(jnp.exp(cum))
    d = expand(jnp.exp(cum[TOK - 1 :] - cum))
    dyb, ub = dy.astype(BF16), u.astype(BF16)
    scores = dot(q, keys)
    du_far = d * dot(keys, g_out, 0, 0)
    dc = jnp.zeros((TOK, TOK), F32)
    ys, dus, diffs = [], [], []
    for h in range(R):
        at = slice(HEAD * h, HEAD * (h + 1))
        mask = masks_of(cum, cum_t, h)
        z = dot(dyb[:, at], ub[:, at], 1, 1)
        lz = mask * z
        dc = dc + lz
        m = lz * scores
        diffs.append(jnp.sum(m.T - m, axis=0, keepdims=True))
        lc = (mask * scores).astype(BF16)
        ys.append(dot(lc, ub[:, at]))
        dus.append(dot(lc, dyb[:, at], 0, 0))
    y = jnp.concatenate(ys, axis=1)
    du = du_far + jnp.concatenate(dus, axis=1)
    pick = head_pick()
    from_d = dot(pick, u * du_far, 1, 1, HIGH)
    dcum = jnp.concatenate(diffs, axis=0) - from_d
    dtot = jnp.sum(from_d, axis=1, keepdims=True)
    gain = sigmoid(tpre)
    dla = dot(dcum, later_mask(), precision=HIGH) + dtot
    dstep = dot(pick, du * vw, 1, 1, HIGH) - rate * dla
    tau = joined(got, NS)
    yi = lax.axis_index("y")
    since = jnp.sum(jnp.where(iota2((Y, HP), 0) < yi, tau, 0.0), axis=0, keepdims=True)
    return (
        (du * stepw).astype(BF16),
        dot(dc.astype(BF16), keys, 1, 1),
        dstep * gain,
        rate * gain,
        y,
        a * (sig * (1.0 + g * (1.0 - sig))),
        e,
        (dy * e).astype(BF16),
        jnp.exp(since),
        expand(jnp.exp(cum[TOK - 1 :])),
    )


def head_pick():
    return (lax.div(iota2((R, HP), 1), HEAD) == iota2((R, HP), 0)).astype(F32)


def later_mask():
    return (iota2((TOK, TOK), 0) >= iota2((TOK, TOK), 1)).astype(F32)


def finish_far(got, near, q, dq_in, dstep, coef, y_in, slope, e, dye, since, total):
    flat = got.reshape(got.shape[0] * PAD, STATE)
    rows = flat.shape[0]
    each = NS // lax.axis_size("z")
    n, col = iota2((STATE, rows), 0), iota2((STATE, rows), 1)
    inner = lax.rem(n, NS)
    source = lax.div(inner, each) * Y + lax.div(n, NS)
    place = source * PAD + lax.rem(inner, each)
    s_in = jnp.concatenate(
        [dot((col == place + each * half).astype(BF16), flat) for half in range(2)], axis=1
    )
    within = lax.rem(iota2((PAD, rows), 1), PAD)
    chosen = ((within >= 4) & (within < 7)).astype(BF16)
    squares = dot(chosen, flat)[:1]
    begin = jnp.concatenate([near[i, 3 * NS :] for i in range(Y)], axis=0).astype(F32)
    s_in = (s_in * since + begin).astype(BF16)
    g_out = jnp.concatenate([near[i, 2 * NS : 3 * NS] for i in range(Y)], axis=0)
    read = dot(q, s_in)
    gate_grad = (slope * (y_in + e * read)).astype(BF16)
    query_grad = (dq_in + dot(dye, s_in, 1, 1)).astype(BF16)
    pick = head_pick()
    from_e = dot(pick, dye.astype(F32) * read, 1, 1, HIGH)
    kept = jnp.sum(s_in.astype(F32) * g_out.astype(F32), axis=0, keepdims=True) * total
    extra = dot(from_e, later_mask(), precision=HIGH) + jnp.sum(
        pick * kept, axis=1, keepdims=True
    )
    return squares, query_grad, dstep - coef * extra, gate_grad


def summed(parts):
    acc = parts[0].astype(F32)
    for i in range(1, parts.shape[0]):
        acc = acc + parts[i].astype(F32)
    return acc


def weight_sum(near, far):
    acc = summed(near[:, :NS])
    squares = split3(jnp.sum(acc * acc, axis=0, keepdims=True))
    count = near.shape[0]
    each = NS // count
    tau = jnp.exp(joined(far, NS))
    row = iota2((PAD, STATE), 0)
    marks = jnp.zeros((PAD, STATE), F32)
    for i, part in enumerate(squares):
        marks = jnp.where(row == 4 + i, part.astype(F32), marks)
    state = jnp.zeros((PAD, STATE), F32)
    blocks = []
    for i in range(count):
        blocks += [(state + marks).astype(BF16)] * Y
        decay = jnp.where(row < each, tau[i : i + 1, :STATE], tau[i : i + 1, STATE:])
        state = decay * state + near[i, NS:].astype(F32)
    return acc, jnp.stack(blocks)


def partial_input(w, own, after):
    edge = lax.axis_index("y") == Y - 1
    spot = iota2((PAD, TOK), 1) == iota2((PAD, TOK), 0) + (TOK - PAD)
    spread = dot(after, spot.astype(F32), 0, 0, HIGH)
    grad = (own + jnp.where(edge, spread, 0.0)).astype(BF16)
    place = lax.axis_index("tp")
    width = w.shape[1] // lax.axis_size("tp")
    core = lax.rem(place, 2)
    chip = lax.div(place, 2)
    near = jnp.bitwise_xor(chip, 1)
    chips = (chip, 3 - chip, near, 3 - near)
    res = []
    for owner in (core, 1 - core):
        blocks = []
        for other in chips:
            rank = other * 2 + owner
            blocks.append(dot(columns_at(w, rank * width, width), grad, 0, 0).astype(BF16))
        res.append(jnp.stack(blocks))
    return res


def half_sum(mine, other):
    size = mine.shape[0] // 2
    total = (mine.astype(F32) + other.astype(F32)).astype(BF16)
    return total[:size], total[size:]


def last_sum(mine, other):
    return (mine[0].astype(F32) + other[0].astype(F32)).astype(BF16)


def exchange(parts, axis):
    return lax.all_to_all(parts, axis, split_axis=0, concat_axis=0, tiled=True)


def around(parts, axis, step):
    count = lax.axis_size(axis)
    ring = count // step
    got = [parts[0]]
    for d in range(1, ring):
        route = [(i, (i + d * step) % count) for i in range(count)]
        got.append(lax.ppermute(parts[d], axis, route))
    return got


def per_device(
    block_source,
    address_weights,
    causal_filter_taps,
    payload_vectors,
    probe_vectors,
    interval_preimage,
    channel_damping_exponent,
    added_damping_jumps,
    sigmoid_argument,
    adjoint_of_result,
):
    return step(
        block_source,
        address_weights,
        causal_filter_taps,
        payload_vectors,
        probe_vectors,
        interval_preimage.T,
        channel_damping_exponent.reshape(1, R),
        added_damping_jumps.T,
        sigmoid_argument,
        adjoint_of_result,
    )


def step(x, w, taps, v, q, tpre, aexp, jump, gate, adj):
    zs = lax.axis_size("z")
    sp = zs * Y
    tp = lax.axis_size("tp")
    features = x.shape[1]
    small = (tpre, aexp, jump, gate, adj)
    bwd_send = local(bwd_local, sds((Y, NS + PAD + TOK, HP), BF16), *small, q, v, vmem=BIG)
    got = exchange(bwd_send, "y")
    rim = lax.ppermute(x[TOK - PAD :], ZY, [(i, i + 1) for i in range(sp - 1)])
    rows = TOK + NS + features // Y // 2 + 2 * PAD
    *mids, keys = local(
        fwd_local,
        [sds((rows, HP), BF16)] * Y + [sds((STATE, TOK), BF16)],
        *small,
        q,
        v,
        x,
        w,
        rim,
        taps,
    )
    mids = around(mids, "y", 1)
    bwd_totals = local(bwd_group, sds((zs, NS + PAD, HP), BF16), got)
    far = exchange(bwd_totals, "z")
    ends = local(bwd_far, sds((Y, 4 * NS, HP), BF16), far, got, *mids)
    ends = exchange(ends, "y")
    send, own, over = local(
        key_grads,
        [sds((zs, NS + PAD, STATE), BF16), sds((STATE, TOK), F32), sds((PAD, STATE), F32)],
        ends,
        got,
        *mids,
        taps,
    )
    near = exchange(send, "z")
    after = lax.ppermute(over, "z", [(i, i - 1) for i in range(1, zs)])
    wide = sds((TOK, HP), F32)
    value_grad, dq_in, dstep, coef, y_in, slope, e, dye, since, total = local(
        finish_near,
        [
            sds((TOK, HP), BF16),
            sds((TOK, STATE), F32),
            sds((R, TOK), F32),
            sds((R, TOK), F32),
            wide,
            wide,
            wide,
            sds((TOK, HP), BF16),
            sds((1, HP), F32),
            sds((1, HP), F32),
        ],
        ends,
        got,
        *small,
        q,
        v,
        keys,
    )
    weight_t, squares = local(
        weight_sum, [sds((NS, STATE), F32), sds((sp, PAD, STATE), BF16)], near, far
    )
    squares = exchange(squares, ZY)
    share = (features // tp, TOK)
    keep, give = local(partial_input, [sds((4, *share), BF16)] * 2, w, own, after, raw=(0,))
    give = lax.ppermute(give, "tp", [(i, i ^ 1) for i in range(tp)])
    keep, give = local(half_sum, [sds((2, *share), BF16)] * 2, keep, give)
    give = lax.ppermute(give, "tp", [(i, i ^ 2) for i in range(tp)])
    keep, give = local(half_sum, [sds((1, *share), BF16)] * 2, keep, give)
    give = lax.ppermute(give, "tp", [(i, i ^ 6) for i in range(tp)])
    input_grad = local(last_sum, sds(share, BF16), keep, give)
    row_squares, query_grad, decay_grad, gate_grad = local(
        finish_far,
        [
            sds((1, STATE), F32),
            sds((TOK, STATE), BF16),
            sds((R, TOK), F32),
            sds((TOK, HP), BF16),
        ],
        squares,
        ends,
        q,
        dq_in,
        dstep,
        coef,
        y_in,
        slope,
        e,
        dye,
        since,
        total,
    )
    return (
        weight_t.T,
        row_squares.reshape(STATE),
        input_grad,
        value_grad,
        query_grad,
        decay_grad.T,
        gate_grad,
    )


def solution(mesh):
    sp, tp = mesh.shape["sp"], mesh.shape["tp"]
    fine = Mesh(mesh.devices.reshape(sp // Y, Y, tp), ("z", "y", "tp"))
    sh = P(ZY, "tp")
    in_specs = (
        P(ZY, None),
        P("tp", None),
        P(None, "tp"),
        sh,
        sh,
        sh,
        P("tp"),
        sh,
        sh,
        sh,
    )
    out_specs = (P("tp", ZY), P("tp"), P("tp", ZY), sh, sh, sh, sh)
    return jax.shard_map(
        per_device, mesh=fine, in_specs=in_specs, out_specs=out_specs, check_vma=False
    )
```

```python
import jax
import jax.numpy as jnp
from jax import lax
from jax.experimental import pallas as pl
from jax.experimental.pallas import tpu as pltpu
from jax.sharding import Mesh
from jax.sharding import PartitionSpec as P


TOK = 128
STATE = 128
HEAD = 64
R = 4
HP = R * HEAD
Y = 4
NS = STATE // Y
PAD = 8
HIGH = lax.Precision.HIGHEST
F32 = jnp.float32
BF16 = jnp.bfloat16
PALLAS = True
Z = ("zh", "zl")
ALL = ("zh", "zl", "y")
VMEM_LIMIT = 16 * 2**20
BIG = 60 * 1024 * 2**10


def dot(a, b, ca=1, cb=0, precision=None):
    return lax.dot_general(
        a, b, (((ca,), (cb,)), ((), ())), preferred_element_type=F32, precision=precision
    )


def roll(a, shift):
    size = a.shape[1]
    if PALLAS:
        return pltpu.roll(a, shift % size, 1)
    return jnp.roll(a, shift, axis=1)


def local(fn, outs, *args, flops=10**7, raw=(), vmem=VMEM_LIMIT):
    single = not isinstance(outs, (list, tuple))
    shapes = [outs] if single else list(outs)
    if not PALLAS:
        res = fn(*args)
        res = [res] if single else list(res)
        for r, s in zip(res, shapes):
            assert r.shape == s.shape and r.dtype == s.dtype, (fn, r, s)
        return res[0] if single else res

    def kernel(*refs):
        ins, dst = refs[: len(args)], refs[len(args) :]
        res = fn(*[r if i in raw else r[...] for i, r in enumerate(ins)])
        res = [res] if single else res
        for ref, val in zip(dst, res):
            ref[...] = val

    vm = pl.BlockSpec(memory_space=pltpu.VMEM)
    res = pl.pallas_call(
        kernel,
        out_shape=shapes,
        in_specs=[vm] * len(args),
        out_specs=[vm] * len(shapes),
        cost_estimate=pl.CostEstimate(flops=flops, bytes_accessed=10**6, transcendentals=0),
        compiler_params=pltpu.CompilerParams(vmem_limit_bytes=vmem),
    )(*args)
    return res[0] if single else res


def sds(shape, dtype):
    return jax.ShapeDtypeStruct(shape, dtype)


def choose(parts, index):
    res = parts[0]
    for i in range(1, len(parts)):
        res = jnp.where(index == i, parts[i], res)
    return res


def to_peers(parts):
    yi = lax.axis_index("y")
    return [choose(parts, lax.rem(yi + d, Y)) for d in range(Y)]


def from_peers(parts):
    yi = lax.axis_index("y")
    return [choose(parts, lax.rem(yi + Y - j, Y)) for j in range(Y)]


def columns_at(ref, start, size):
    if PALLAS:
        return ref[:, pl.ds(pl.multiple_of(start, size), size)]
    return lax.dynamic_slice_in_dim(ref, start, size, axis=1)


def iota2(shape, dim):
    return lax.broadcasted_iota(jnp.int32, shape, dim)


def expand(a):
    return jnp.concatenate(
        [jnp.broadcast_to(a[:, h : h + 1], (a.shape[0], HEAD)) for h in range(R)], axis=1
    )


def split3(a):
    hi = a.astype(BF16)
    rest = a - hi.astype(F32)
    mid = rest.astype(BF16)
    low = (rest - mid.astype(F32)).astype(BF16)
    return hi, mid, low


def joined(parts, first):
    return (
        parts[:, first].astype(F32)
        + parts[:, first + 1].astype(F32)
        + parts[:, first + 2].astype(F32)
    )


def column(a):
    eye = (iota2((TOK, TOK), 0) == iota2((TOK, TOK), 1)).astype(F32)
    return dot(eye, a, 1, 1, HIGH)


def decays(tpre, aexp, jump):
    step = jnp.log(1.0 + jnp.exp(tpre))
    same = iota2((R, R), 0) == iota2((R, R), 1)
    rate = jnp.sum(jnp.where(same, jnp.exp(aexp), 0.0), axis=1, keepdims=True)
    la = jump - rate * step
    tri = (iota2((TOK, TOK), 0) >= iota2((TOK, TOK), 1)).astype(F32)
    cum = dot(tri, la, 1, 1, HIGH)
    return step, rate, la, cum


def row_form(la):
    upper = (iota2((TOK, TOK), 0) <= iota2((TOK, TOK), 1)).astype(F32)
    return dot(la, upper, precision=HIGH)


def sigmoid(v):
    return 1.0 / (1.0 + jnp.exp(-v))


def bwd_local(tpre, aexp, jump, gate, adj, q, v):
    step, _, _, cum = decays(tpre, aexp, jump)
    g = gate.astype(F32)
    dy = adj.astype(F32) * g * sigmoid(g)
    dye = (dy * expand(jnp.exp(cum))).astype(BF16)
    lg = dot(q, dye, 0, 0).astype(BF16)
    ud = v.astype(F32) * expand(column(step) * jnp.exp(cum[TOK - 1 :] - cum))
    hi, mid, low = split3(expand(cum[TOK - 1 :]))
    tail = jnp.concatenate(
        [hi, mid, low, jnp.zeros((PAD - 3, HP), BF16), ud.astype(BF16)], axis=0
    )
    return jnp.stack([jnp.concatenate([lg[NS * i : NS * (i + 1)], tail], axis=0) for i in range(Y)])


def masks_of(cum, cum_t, h):
    causal = iota2((TOK, TOK), 0) >= iota2((TOK, TOK), 1)
    return jnp.exp(jnp.where(causal, cum[:, h : h + 1] - cum_t[h : h + 1, :], -1e30))


def fwd_local(tpre, aexp, jump, gate, adj, q, v, x, w, rim, taps):
    step, _, la, cum = decays(tpre, aexp, jump)
    cum_t = row_form(la)
    taps_t = column(taps)
    rim = jnp.where(iota2(rim.shape, 0) >= PAD - 3, rim.astype(F32), 0.0).astype(BF16)
    g = gate.astype(F32)
    dy = (adj.astype(F32) * g * sigmoid(g)).astype(BF16)
    u = v.astype(F32) * expand(column(step))
    ud = (u * expand(jnp.exp(cum[TOK - 1 :] - cum))).astype(BF16)
    u = u.astype(BF16)
    dc = jnp.zeros((TOK, TOK), F32)
    for h in range(R):
        at = slice(HEAD * h, HEAD * (h + 1))
        dc = dc + masks_of(cum, cum_t, h) * dot(dy[:, at], u[:, at], 1, 1)
    dki = dot(q, dc.astype(BF16), 0, 0)
    proj = dot(w, x, 1, 1).astype(BF16).astype(F32)
    rim_proj = dot(w, rim, 1, 1).astype(BF16)
    place = (iota2((PAD, TOK), 1) == iota2((PAD, TOK), 0) + (TOK - PAD)).astype(BF16)
    rim_full = dot(rim_proj, place)
    lane = iota2((STATE, TOK), 1)
    conv = taps_t[:, 3:4] * proj
    for d in range(1, 4):
        conv = conv + taps_t[:, 3 - d : 4 - d] * roll(
            jnp.where(lane >= TOK - d, rim_full, proj), d
        )
    sig = sigmoid(conv)
    keys = (conv * sig).astype(BF16)
    slope = sig * (1.0 + conv * (1.0 - sig))
    ls = dot(keys, ud).astype(BF16)
    pair = jnp.concatenate([dki.astype(BF16), slope.astype(BF16)], axis=1)
    eye = (iota2((TOK, TOK), 0) == iota2((TOK, TOK), 1)).astype(BF16)
    xt = dot(x, eye, 0, 0).astype(BF16)
    small_eye = (iota2((PAD, PAD), 0) == iota2((PAD, PAD), 1)).astype(BF16)
    rt = dot(rim, small_eye, 0, 0).astype(BF16)
    width = Y * NS
    blocks = x.shape[1] // width

    def features_of(a, i):
        return jnp.concatenate(
            [a[width * b + NS * i : width * b + NS * (i + 1)] for b in range(blocks)], axis=0
        )

    own = []
    for i in range(Y):
        xs = features_of(xt, i)
        rs = dot(small_eye, features_of(rt, i), 1, 1).astype(BF16)
        half = xs.shape[0] // 2
        xs = jnp.concatenate([xs[:half], xs[half:]], axis=1)
        own.append(jnp.concatenate([xs, rs[:, :half], rs[:, half:]], axis=0))
    return *[jnp.concatenate([pair, ls, part], axis=0) for part in to_peers(own)], keys


def folded(parts, tau):
    acc = parts[-1, :NS].astype(F32)
    for j in range(parts.shape[0] - 2, -1, -1):
        acc = parts[j, :NS].astype(F32) + jnp.exp(tau[j : j + 1]) * acc
    return acc.astype(BF16)


def bwd_group(got):
    tau = joined(got, NS)
    marks = split3(jnp.sum(tau, axis=0, keepdims=True))
    part = jnp.concatenate(
        [folded(got, tau), *marks, jnp.zeros((PAD - 3, HP), BF16)], axis=0
    )
    return jnp.stack([part] * lax.axis_size("zl"))


def bwd_quad(near):
    tau = joined(near, NS)
    count = near.shape[0]
    marks = [m for j in range(count) for m in split3(tau[j : j + 1])[:2]]
    part = jnp.concatenate([folded(near, tau), *marks], axis=0)
    return jnp.stack([part] * lax.axis_size("zh"))


def own_group(got):
    return joined(got, NS)


def paired(parts, first):
    return parts[:, first].astype(F32) + parts[:, first + 1].astype(F32)


def suffix(parts, tau, mine, state):
    for i in range(parts.shape[0] - 1, -1, -1):
        longer = parts[i, :NS].astype(F32) + jnp.exp(tau[i : i + 1]) * state
        state = jnp.where(i > mine, longer, state)
    return state


def bwd_far(far, close, got):
    tau = paired(far, NS)
    for j in range(1, close.shape[0]):
        tau = tau + paired(far, NS + 2 * j)
    state = suffix(far, tau, lax.axis_index("zh"), jnp.zeros((NS, HP), F32))
    state = suffix(close, joined(close, NS), lax.axis_index("zl"), state)
    decay = jnp.exp(joined(got, NS))
    ends = [None] * Y
    for j in range(Y - 1, -1, -1):
        ends[j] = state.astype(BF16)
        if j:
            state = got[j, :NS].astype(F32) + decay[j : j + 1] * state
    dk = [dot(ends[j], got[j, NS + PAD :], 1, 1).astype(BF16) for j in range(Y)]
    pairs = [jnp.concatenate(dk[i : i + 2], axis=1) for i in range(0, Y, 2)]
    return jnp.stack([jnp.concatenate([*pairs, ends[j]], axis=0) for j in range(Y)])


def key_grads(near, got, m0, m1, m2, m3, taps):
    yi = lax.axis_index("y")
    mids = (m0, m1, m2, m3)
    first = 2 * TOK
    last = m0.shape[0] - 2 * PAD
    mid = from_peers([m[:first] for m in mids])
    edge = choose([m[last:] for m in mids], yi)
    taps_t = column(taps)
    dk = jnp.concatenate(
        [
            jnp.concatenate([near[i, :NS], near[i, NS : 2 * NS]], axis=1)
            for i in range(Y)
        ],
        axis=0,
    ).astype(F32)
    dki = jnp.concatenate([part[:STATE, :TOK] for part in mid], axis=1).astype(F32)
    slope = jnp.concatenate([part[:STATE, TOK:] for part in mid], axis=1).astype(F32)
    cg = (dk + dki) * slope
    size = Y * TOK
    lane = iota2((STATE, size), 1)
    main = taps_t[:, 3:4] * cg
    over = jnp.zeros_like(main)
    for d in range(1, 4):
        moved = taps_t[:, 3 - d : 4 - d] * roll(cg, -d)
        main = main + jnp.where(lane < size - d, moved, 0.0)
        over = over + jnp.where(lane >= size - d, moved, 0.0)
    over = over[:, size - TOK :]
    pg = main.astype(BF16)
    rims = jnp.concatenate([edge[:PAD], edge[PAD:]], axis=1)
    dw = dot(rims, over[:, TOK - PAD :].astype(BF16), 0, 1)
    pg = [pg[:, TOK * j : TOK * (j + 1)] for j in range(Y)]
    for d, part in enumerate(mids):
        xs = jnp.concatenate([part[first:last, :TOK], part[first:last, TOK:]], axis=0)
        dw = dw + dot(xs, choose(pg, lax.rem(yi + Y - d, Y)), 1, 1)
    dw = dw.astype(BF16)
    decay = jnp.exp(own_group(got))
    fwd = mid[0][TOK:first].astype(F32)
    for j in range(1, Y):
        fwd = mid[j][TOK:first].astype(F32) + decay[j : j + 1] * fwd
    fwd = choose([fwd[NS * i : NS * (i + 1)] for i in range(Y)], yi).astype(BF16)
    count = dw.shape[0] // NS
    each = NS // count
    row, col = iota2((PAD * count, NS), 0), iota2((PAD * count, NS), 1)
    part = lax.rem(row, PAD)
    target = lax.div(row, PAD) * each + lax.rem(part, each)
    tail = jnp.zeros((PAD * count, STATE), F32)
    for half in range(2):
        pick = (col == target) & (lax.div(part, each) == half)
        tail = tail + dot(pick.astype(BF16), fwd[:, STATE * half : STATE * (half + 1)])
    tail = tail.astype(BF16)
    send = jnp.stack(
        [
            jnp.concatenate(
                [dw[NS * i : NS * (i + 1)], tail[PAD * i : PAD * (i + 1)]], axis=0
            )
            for i in range(count)
        ]
    )
    own = choose([main[:, TOK * j : TOK * (j + 1)] for j in range(Y)], yi)
    eye = (iota2((PAD, PAD), 0) == iota2((PAD, PAD), 1)).astype(F32)
    return send, own, dot(eye, over[:, TOK - PAD :], 1, 1, HIGH)


def finish_near(near, got, m0, m1, m2, m3, tpre, aexp, jump, gate, adj, q, v, keys):
    step, rate, la, cum = decays(tpre, aexp, jump)
    cum_t = row_form(la)
    g_out = jnp.concatenate([near[i, 2 * NS :] for i in range(Y)], axis=0)
    g = gate.astype(F32)
    a = adj.astype(F32)
    sig = sigmoid(g)
    dy = a * g * sig
    vw = v.astype(F32)
    stepw = expand(column(step))
    u = vw * stepw
    e = expand(jnp.exp(cum))
    d = expand(jnp.exp(cum[TOK - 1 :] - cum))
    dyb, ub = dy.astype(BF16), u.astype(BF16)
    scores = dot(q, keys)
    du_far = d * dot(keys, g_out, 0, 0)
    dc = jnp.zeros((TOK, TOK), F32)
    ys, dus, diffs = [], [], []
    for h in range(R):
        at = slice(HEAD * h, HEAD * (h + 1))
        mask = masks_of(cum, cum_t, h)
        z = dot(dyb[:, at], ub[:, at], 1, 1)
        lz = mask * z
        dc = dc + lz
        m = lz * scores
        diffs.append(jnp.sum(m.T - m, axis=0, keepdims=True))
        lc = (mask * scores).astype(BF16)
        ys.append(dot(lc, ub[:, at]))
        dus.append(dot(lc, dyb[:, at], 0, 0))
    y = jnp.concatenate(ys, axis=1)
    du = du_far + jnp.concatenate(dus, axis=1)
    pick = head_pick()
    from_d = dot(pick, u * du_far, 1, 1, HIGH)
    dcum = jnp.concatenate(diffs, axis=0) - from_d
    dtot = jnp.sum(from_d, axis=1, keepdims=True)
    gain = sigmoid(tpre)
    dla = dot(dcum, later_mask(), precision=HIGH) + dtot
    dstep = dot(pick, du * vw, 1, 1, HIGH) - rate * dla
    tau = own_group(got)
    yi = lax.axis_index("y")
    mid = from_peers([m[TOK : 2 * TOK] for m in (m0, m1, m2, m3)])
    begin = jnp.zeros((STATE, HP), F32)
    for j in range(Y - 1):
        after = mid[j].astype(F32) + jnp.exp(tau[j : j + 1]) * begin
        begin = jnp.where(j < yi, after, begin)
    since = jnp.sum(jnp.where(iota2((Y, HP), 0) < yi, tau, 0.0), axis=0, keepdims=True)
    return (
        (du * stepw).astype(BF16),
        dot(dc.astype(BF16), keys, 1, 1),
        dstep * gain,
        rate * gain,
        y,
        a * (sig * (1.0 + g * (1.0 - sig))),
        e,
        (dy * e).astype(BF16),
        jnp.exp(since),
        expand(jnp.exp(cum[TOK - 1 :])),
        begin.astype(BF16),
    )


def head_pick():
    return (lax.div(iota2((R, HP), 1), HEAD) == iota2((R, HP), 0)).astype(F32)


def later_mask():
    return (iota2((TOK, TOK), 0) >= iota2((TOK, TOK), 1)).astype(F32)


def finish_far(got, near, q, dq_in, dstep, coef, y_in, slope, e, dye, since, total, begin):
    flat = got.reshape(got.shape[0] * PAD, STATE)
    rows = flat.shape[0]
    each = NS // (lax.axis_size("zh") * lax.axis_size("zl"))
    n, col = iota2((STATE, rows), 0), iota2((STATE, rows), 1)
    inner = lax.rem(n, NS)
    source = lax.div(inner, each) * Y + lax.div(n, NS)
    place = source * PAD + lax.rem(inner, each)
    s_in = jnp.concatenate(
        [dot((col == place + each * half).astype(BF16), flat) for half in range(2)], axis=1
    )
    within = lax.rem(iota2((PAD, rows), 1), PAD)
    chosen = ((within >= 4) & (within < 7)).astype(BF16)
    squares = dot(chosen, flat)[:1]
    s_in = (s_in * since + begin.astype(F32)).astype(BF16)
    g_out = jnp.concatenate([near[i, 2 * NS :] for i in range(Y)], axis=0)
    read = dot(q, s_in)
    gate_grad = (slope * (y_in + e * read)).astype(BF16)
    query_grad = (dq_in + dot(dye, s_in, 1, 1)).astype(BF16)
    pick = head_pick()
    from_e = dot(pick, dye.astype(F32) * read, 1, 1, HIGH)
    kept = jnp.sum(s_in.astype(F32) * g_out.astype(F32), axis=0, keepdims=True) * total
    extra = dot(from_e, later_mask(), precision=HIGH) + jnp.sum(
        pick * kept, axis=1, keepdims=True
    )
    return squares, query_grad, dstep - coef * extra, gate_grad


def summed(parts):
    acc = parts[0].astype(F32)
    for i in range(1, parts.shape[0]):
        acc = acc + parts[i].astype(F32)
    return acc


def weight_sum(near, far):
    acc = summed(near[:, :NS])
    squares = split3(jnp.sum(acc * acc, axis=0, keepdims=True))
    count = near.shape[0]
    each = NS // count
    inner = lax.axis_size("zl")
    tau = [jnp.exp(paired(far, NS + 2 * j)) for j in range(inner)]
    row = iota2((PAD, STATE), 0)
    marks = jnp.zeros((PAD, STATE), F32)
    for i, part in enumerate(squares):
        marks = jnp.where(row == 4 + i, part.astype(F32), marks)
    state = jnp.zeros((PAD, STATE), F32)
    blocks = []
    for i in range(count):
        blocks += [(state + marks).astype(BF16)] * Y
        here = tau[i % inner][i // inner : i // inner + 1]
        decay = jnp.where(row < each, here[:, :STATE], here[:, STATE:])
        state = decay * state + near[i, NS:].astype(F32)
    return acc, jnp.stack(blocks)


def partial_input(w, own, after):
    edge = lax.axis_index("y") == Y - 1
    spot = iota2((PAD, TOK), 1) == iota2((PAD, TOK), 0) + (TOK - PAD)
    spread = dot(after, spot.astype(F32), 0, 0, HIGH)
    grad = (own + jnp.where(edge, spread, 0.0)).astype(BF16)
    place = lax.axis_index("tp")
    width = w.shape[1] // lax.axis_size("tp")
    core = lax.rem(place, 2)
    chip = lax.div(place, 2)
    near = jnp.bitwise_xor(chip, 1)
    chips = (chip, 3 - chip, near, 3 - near)
    res = []
    for owner in (core, 1 - core):
        blocks = []
        for other in chips:
            rank = other * 2 + owner
            blocks.append(dot(columns_at(w, rank * width, width), grad, 0, 0).astype(BF16))
        res.append(jnp.stack(blocks))
    return res


def half_sum(mine, other):
    size = mine.shape[0] // 2
    total = (mine.astype(F32) + other.astype(F32)).astype(BF16)
    return total[:size], total[size:]


def last_sum(mine, other):
    return (mine[0].astype(F32) + other[0].astype(F32)).astype(BF16)


def exchange(parts, axis):
    return lax.all_to_all(parts, axis, split_axis=0, concat_axis=0, tiled=True)


def around(parts, axis):
    count = lax.axis_size(axis)
    got = [parts[0]]
    for d in range(1, count):
        got.append(lax.ppermute(parts[d], axis, [(i, (i + d) % count) for i in range(count)]))
    return got


def per_device(
    block_source,
    address_weights,
    causal_filter_taps,
    payload_vectors,
    probe_vectors,
    interval_preimage,
    channel_damping_exponent,
    added_damping_jumps,
    sigmoid_argument,
    adjoint_of_result,
):
    return step(
        block_source,
        address_weights,
        causal_filter_taps,
        payload_vectors,
        probe_vectors,
        interval_preimage.T,
        channel_damping_exponent.reshape(1, R),
        added_damping_jumps.T,
        sigmoid_argument,
        adjoint_of_result,
    )


def step(x, w, taps, v, q, tpre, aexp, jump, gate, adj):
    far_count = lax.axis_size("zh")
    zs = far_count * lax.axis_size("zl")
    sp = zs * Y
    tp = lax.axis_size("tp")
    features = x.shape[1]
    small = (tpre, aexp, jump, gate, adj)
    bwd_send = local(bwd_local, sds((Y, NS + PAD + TOK, HP), BF16), *small, q, v, vmem=BIG)
    got = exchange(bwd_send, "y")
    rim = lax.ppermute(x[TOK - PAD :], ALL, [(i, i + 1) for i in range(sp - 1)])
    rows = 2 * TOK + features // Y // 2 + 2 * PAD
    *mids, keys = local(
        fwd_local,
        [sds((rows, HP), BF16)] * Y + [sds((STATE, TOK), BF16)],
        *small,
        q,
        v,
        x,
        w,
        rim,
        taps,
    )
    mids = around(mids, "y")
    close_count = lax.axis_size("zl")
    totals = local(bwd_group, sds((close_count, NS + PAD, HP), BF16), got)
    close = exchange(totals, "zl")
    marks = 2 * close_count
    totals = local(bwd_quad, sds((far_count, NS + marks, HP), BF16), close)
    far = exchange(totals, "zh")
    ends = local(bwd_far, sds((Y, 3 * NS, HP), BF16), far, close, got)
    ends = exchange(ends, "y")
    send, own, over = local(
        key_grads,
        [sds((zs, NS + PAD, STATE), BF16), sds((STATE, TOK), F32), sds((PAD, STATE), F32)],
        ends,
        got,
        *mids,
        taps,
    )
    near = exchange(send, Z)
    after = lax.ppermute(over, Z, [(i, i - 1) for i in range(1, zs)])
    wide = sds((TOK, HP), F32)
    value_grad, dq_in, dstep, coef, y_in, slope, e, dye, since, total, begin = local(
        finish_near,
        [
            sds((TOK, HP), BF16),
            sds((TOK, STATE), F32),
            sds((R, TOK), F32),
            sds((R, TOK), F32),
            wide,
            wide,
            wide,
            sds((TOK, HP), BF16),
            sds((1, HP), F32),
            sds((1, HP), F32),
            sds((STATE, HP), BF16),
        ],
        ends,
        got,
        *mids,
        *small,
        q,
        v,
        keys,
    )
    weight_t, squares = local(
        weight_sum, [sds((NS, STATE), F32), sds((sp, PAD, STATE), BF16)], near, far
    )
    squares = exchange(squares, ALL)
    share = (features // tp, TOK)
    keep, give = local(partial_input, [sds((4, *share), BF16)] * 2, w, own, after, raw=(0,))
    give = lax.ppermute(give, "tp", [(i, i ^ 1) for i in range(tp)])
    keep, give = local(half_sum, [sds((2, *share), BF16)] * 2, keep, give)
    give = lax.ppermute(give, "tp", [(i, i ^ 2) for i in range(tp)])
    keep, give = local(half_sum, [sds((1, *share), BF16)] * 2, keep, give)
    give = lax.ppermute(give, "tp", [(i, i ^ 6) for i in range(tp)])
    input_grad = local(last_sum, sds(share, BF16), keep, give)
    row_squares, query_grad, decay_grad, gate_grad = local(
        finish_far,
        [
            sds((1, STATE), F32),
            sds((TOK, STATE), BF16),
            sds((R, TOK), F32),
            sds((TOK, HP), BF16),
        ],
        squares,
        ends,
        q,
        dq_in,
        dstep,
        coef,
        y_in,
        slope,
        e,
        dye,
        since,
        total,
        begin,
    )
    return (
        weight_t.T,
        row_squares.reshape(STATE),
        input_grad,
        value_grad,
        query_grad,
        decay_grad.T,
        gate_grad,
    )


def solution(mesh):
    sp, tp = mesh.shape["sp"], mesh.shape["tp"]
    fine = Mesh(mesh.devices.reshape(sp // (4 * Y), 4, Y, tp), (*ALL, "tp"))
    sh = P(ALL, "tp")
    in_specs = (
        P(ALL, None),
        P("tp", None),
        P(None, "tp"),
        sh,
        sh,
        sh,
        P("tp"),
        sh,
        sh,
        sh,
    )
    out_specs = (P("tp", ALL), P("tp"), P("tp", ALL), sh, sh, sh, sh)
    return jax.shard_map(
        per_device, mesh=fine, in_specs=in_specs, out_specs=out_specs, check_vma=False
    )
```
